32 devices in a mesh: sp: 8 (over z, x), tp: 4 (over y, core).
Axes of the slice: x: 2, y: 2, z: 4, core: 2. Of those that a mesh axis runs over, the one named last changes fastest.
Arguments:
- saved_tokens: bfloat16 [1536, 2048], P('sp'), may hold values from -3.75 to 3.75
- cotangent: bfloat16 [1536, 2048], P('sp'), may hold values from -6 to 6
- routes: int32 [1536, 2], P('sp'), may hold values from 0 to 7, all different within a row; in each aligned block of 192 rows (0 to 191, 192 to 383, ...) at most 96 rows name the same one
- route_weights: float32 [1536, 2], P('sp'), may hold values from 0.2 to 1
- gate_in: bfloat16 [1536, 1024], P('sp', 'tp'), may hold values from -6 to 6
- conv_in: bfloat16 [1536, 1024], P('sp', 'tp'), may hold values from -6 to 6
- value_in: bfloat16 [1536, 1024], P('sp', 'tp'), may hold values from -6 to 6
- conv_taps: float32 [3, 1024], replicated, may hold values from -3.5 to 3.5
- out_weight: bfloat16 [2048, 1024], P(None, 'tp'), may hold values from -0.1875 to 0.1875
- gate_proj: bfloat16 [8, 2048, 2048], P('sp', None, 'tp'), may hold values from -0.125 to 0.125
- up_proj: bfloat16 [8, 2048, 2048], P('sp', None, 'tp'), may hold values from -0.125 to 0.125
- down_proj: bfloat16 [8, 2048, 2048], P('sp', 'tp'), may hold values from -0.125 to 0.125
Outputs:
- gate_proj_grad: float32 [8, 2048, 2048], P('sp', None, 'tp')
- up_proj_grad: float32 [8, 2048, 2048], P('sp', None, 'tp')
- down_proj_grad: float32 [8, 2048, 2048], P('sp', 'tp')
- out_weight_grad: float32 [2048, 1024], P('sp', 'tp')
- token_grad: bfloat16 [1536, 2048], P('sp', 'tp')
- gate_in_grad: bfloat16 [1536, 1024], P('sp', 'tp')
- conv_in_grad: bfloat16 [1536, 1024], P('sp', 'tp')
- value_in_grad: bfloat16 [1536, 1024], P('sp', 'tp')
The draws below stay inside these ranges and needn't reach their ends.
Inputs may be any that keep to these rules, and one draw needn't show every extreme that they name: `routes`: within each aligned block of 192 tokens at most 96 assignments name one expert, a bound that some block reaches of them; the 2 experts of a token differ.
All inputs are finite; a program needn't handle non-finite values.
Results may differ from the reference program's by a relative error of at most 0.0063.
Values may be sent and summed in bfloat16 or wider, within the bound.
A program may use at most 64 MiB of HBM per device.

```python
import math
import jax
import jax.numpy as jnp
import numpy as np
from jax import lax

D = 2048
FF = 2048
DC = 1024
TAPS = 3
TOP = 2
TOK_DEV = 192
EXPERTS = 8
TOKENS = 1536
CAP = 96
HID_GROUPS = 4
N_SP = 8


def spiked(drawn, stream_key, source, target, shards_of, factor):
    def block_of(axis_at):
        return (jnp.arange(drawn.shape[axis_at]) // (drawn.shape[axis_at] // shards_of)).reshape((-1,) + (1,) * (drawn.ndim - 1 - axis_at))

    first = jax.random.permutation(stream_key, shards_of)[block_of(target)]
    far = (block_of(target) + shards_of // 2) % shards_of
    return jnp.where((block_of(source) == first) | (block_of(source) == far), factor * drawn, drawn)


def steps_of(own_key, dims, shards, low, largest):
    def one(position, shards_of):
        draws = jax.random.uniform(jax.random.fold_in(jax.random.fold_in(own_key, 6), position), (shards_of,), jnp.float32, low / len(shards), largest / len(shards))
        return jnp.repeat(jnp.exp(draws), dims[position] // shards_of).reshape((-1,) + (1,) * (len(dims) - position - 1))

    gain = one(*shards[0])
    for cut in shards[1:]:
        gain = gain * one(*cut)
    return gain


def routed_block(rng, own, number, rows, number_of, top, most, skew):
    sequence = jax.random.permutation(rng, number_of)
    crowded, ordinary = load_shares(number_of, rows * top, most, skew, True), load_shares(number_of, rows * top, most, skew, False)
    places = jnp.arange(number_of)

    def named(lengths, offset_by):
        used = int((lengths > 0).sum())
        fixed = max(1, used // 4)
        shifted = fixed + (places - fixed + offset_by * (used - fixed)) % max(1, number_of - fixed)
        return jnp.zeros((number_of,), jnp.int32).at[sequence[jnp.where(places < fixed, places, shifted)]].set(jnp.asarray(lengths, jnp.int32))

    lengths = jnp.where(number % 4 == 0, named(crowded, number // 4), named(ordinary, number - number // 4 - 1))
    mixed = jax.random.permutation(jax.random.fold_in(own, 3), number_of)
    source_of, taker = mixed[0:number_of // 2 * 2:2], mixed[1:number_of // 2 * 2:2]
    room = jnp.minimum(lengths[source_of] - 1, most - lengths[taker]) // 2
    room = jnp.where((source_of == sequence[0]) | (taker == sequence[0]) | (lengths[taker] == 0), 0, jnp.maximum(room, 0))
    shifted = jax.random.randint(jax.random.fold_in(own, 4), (number_of // 2,), 0, 1 << 20) % (room + 1)
    lengths = lengths.at[source_of].add(-shifted).at[taker].add(shifted)
    items = jnp.searchsorted(jnp.cumsum(lengths), jnp.arange(rows * top), side="right").astype(jnp.int32)
    table = items.reshape(top, rows).T
    table = table[jax.random.permutation(jax.random.fold_in(own, 1), rows)]
    offset_by = jax.random.randint(jax.random.fold_in(own, 2), (rows, 1), 0, top)
    return jnp.take_along_axis(table, (jnp.arange(top)[None, :] + offset_by) % top, axis=1)


def load_shares(number_of, total, most, lean, full):
    portions = [(1 << 20) // math.isqrt(rank ** lean) + 1 for rank in range(1, number_of + 1)]
    largest = most if full else min(most, max(-(-total // number_of), total * portions[0] // sum(portions)))
    least = 1 if total - largest >= number_of - 1 else 0
    holding, spare = [largest] + [least] * (number_of - 1), total - largest - least * (number_of - 1)
    while spare > 0:
        free = [i for i in range(1, number_of) if holding[i] < largest] or [i for i in range(1, number_of) if holding[i] < most]
        pool, budget = sum([portions[i] for i in free]), spare
        for i in free:
            more = min(most - holding[i], max(1, budget * portions[i] // pool), spare)
            holding[i] = holding[i] + more
            spare = spare - more
    return np.array(holding)


def bell_draw(own_key, extent, scale, most, shards=(), kind=jnp.bfloat16):
    array = scale * jax.random.normal(own_key, extent, jnp.float32)
    if shards:
        array = array * steps_of(own_key, extent, shards, -0.22, 0.18)
    return jnp.clip(array, -most, most).astype(kind)


def gaussian_with(stream_key, extent, scale, most, pieces, heavy, kind=jnp.bfloat16):
    values = scale * jax.random.normal(stream_key, extent, jnp.float32)
    if pieces:
        values = values * steps_of(stream_key, extent, pieces, -0.22, 0.18)
    return jnp.clip(spiked(values, jax.random.fold_in(stream_key, 3), *heavy), -most, most).astype(kind)


def setup_inputs(seed: int = 0) -> dict:
    splits = jax.random.split(jax.random.key(seed), 13)
    saved_tokens = bell_draw(splits[0], (TOKENS, D), 1.25, 3.75, ((0, 8),))
    cotangent = gaussian_with(splits[1], (TOKENS, D), 1.0, 6.0, ((0, 8),), (0, 1, 8, 2.0))
    routes_keys = jax.random.split(jax.random.fold_in(splits[2], 1), TOKENS // TOK_DEV)
    routes_turns = jax.random.permutation(jax.random.fold_in(splits[2], 3), TOKENS // TOK_DEV)
    routes = jax.vmap(lambda own, number: routed_block(jax.random.fold_in(splits[2], 2), own, number, TOK_DEV, EXPERTS, TOP, CAP, 1))(routes_keys, routes_turns).reshape((TOKENS, TOP))
    route_weights = jnp.clip(0.2 + 0.8 * jax.random.uniform(splits[3], (TOKENS, TOP), jnp.float32) ** steps_of(splits[3], (TOKENS, TOP), ((0, 8),), -0.2, 0.2), 0.2, 1.0)
    gate_in = bell_draw(splits[4], (TOKENS, DC), 1.0, 6.0, ((0, 8), (1, 4)))
    conv_in = bell_draw(splits[5], (TOKENS, DC), 1.0, 6.0, ((0, 8), (1, 4)))
    value_in = bell_draw(splits[6], (TOKENS, DC), 1.0, 6.0, ((0, 8), (1, 4)))
    conv_taps = bell_draw(splits[7], (TAPS, DC), TAPS ** -0.5, 3.5, (), jnp.float32)
    out_weight = bell_draw(splits[8], (D, DC), DC ** -0.5, 0.1875, ((1, 4),))
    gate_proj = bell_draw(splits[9], (EXPERTS, D, FF), D ** -0.5, 0.125, ((0, 8), (2, 4)))
    up_proj = bell_draw(splits[10], (EXPERTS, D, FF), D ** -0.5, 0.125, ((0, 8), (2, 4)))
    down_proj = bell_draw(splits[11], (EXPERTS, FF, D), FF ** -0.5, 0.125, ((0, 8), (1, 4)))
    return dict(saved_tokens=saved_tokens, cotangent=cotangent, routes=routes, route_weights=route_weights, gate_in=gate_in, conv_in=conv_in, value_in=value_in, conv_taps=conv_taps, out_weight=out_weight, gate_proj=gate_proj, up_proj=up_proj, down_proj=down_proj)


CLAMP_LIMIT = 7.0
SILU_ALPHA = 1.702


def expert_pass(members):
    rows_in, grads_in, w_gate, w_up, w_down = members
    gate_pre = jnp.dot(rows_in, w_gate, preferred_element_type=jnp.float32)
    up_pre = jnp.dot(rows_in, w_up, preferred_element_type=jnp.float32)
    gate_clip = jnp.minimum(gate_pre, CLAMP_LIMIT)
    up_clip = jnp.clip(up_pre, -CLAMP_LIMIT, CLAMP_LIMIT)
    sigmoid_gate = jax.nn.sigmoid(SILU_ALPHA * gate_clip)
    gated_act = gate_clip * sigmoid_gate
    hidden = ((up_clip + 1.0) * gated_act).astype(jnp.bfloat16)
    d_hidden = jnp.dot(grads_in, w_down.T, preferred_element_type=jnp.float32)
    d_up = jnp.where(jnp.abs(up_pre) < CLAMP_LIMIT, d_hidden * gated_act, 0.0).astype(jnp.bfloat16)
    gate_slope = sigmoid_gate + SILU_ALPHA * gate_clip * sigmoid_gate * (1.0 - sigmoid_gate)
    d_gate = jnp.where(gate_pre < CLAMP_LIMIT, d_hidden * (up_clip + 1.0) * gate_slope, 0.0).astype(jnp.bfloat16)
    down_grad = jnp.dot(hidden.T, grads_in, preferred_element_type=jnp.float32)
    gate_grad = jnp.dot(rows_in.T, d_gate, preferred_element_type=jnp.float32)
    up_grad = jnp.dot(rows_in.T, d_up, preferred_element_type=jnp.float32)
    group_width = FF // HID_GROUPS
    slot_count = rows_in.shape[0]
    gate_terms = jnp.einsum('rgf,dgf->grd',
                            d_gate.astype(jnp.float32).reshape(slot_count, HID_GROUPS, group_width),
                            w_gate.astype(jnp.float32).reshape(D, HID_GROUPS, group_width))
    up_terms = jnp.einsum('rgf,dgf->grd',
                          d_up.astype(jnp.float32).reshape(slot_count, HID_GROUPS, group_width),
                          w_up.astype(jnp.float32).reshape(D, HID_GROUPS, group_width))
    rounded = lax.optimization_barrier((gate_terms + up_terms).astype(jnp.bfloat16))
    return gate_grad, up_grad, down_grad, jnp.sum(rounded.astype(jnp.float32), axis=0)


def reference(saved_tokens, cotangent, routes, route_weights, gate_in, conv_in, value_in,
              conv_taps, out_weight, gate_proj, up_proj, down_proj):
    block_assigns = TOK_DEV * TOP
    flat_routes = routes.reshape(N_SP, block_assigns).astype(jnp.int32)
    onehot = (flat_routes[:, :, None] == jnp.arange(EXPERTS, dtype=jnp.int32)[None, None, :]).astype(jnp.int32)
    slot_rank = jnp.sum((jnp.cumsum(onehot, axis=1) - 1) * onehot, axis=2)
    source = jnp.arange(N_SP, dtype=jnp.int32)[:, None]
    slot_index = (flat_routes * (N_SP * CAP) + source * CAP + slot_rank).reshape(-1).astype(jnp.int32)
    total_assigns = TOKENS * TOP
    slot_owner = jnp.full((EXPERTS * N_SP * CAP,), total_assigns, jnp.int32).at[slot_index].set(
        jnp.arange(total_assigns, dtype=jnp.int32))
    zero_row = jnp.zeros((1, D), jnp.bfloat16)
    token_rows = jnp.concatenate([saved_tokens, zero_row], 0)[slot_owner // TOP].reshape(EXPERTS, N_SP * CAP, D)
    scaled = (route_weights[:, :, None] * cotangent.astype(jnp.float32)[:, None, :]).astype(jnp.bfloat16)
    scaled = scaled.reshape(total_assigns, D)
    grad_rows = jnp.concatenate([scaled, zero_row], 0)[slot_owner].reshape(EXPERTS, N_SP * CAP, D)
    gate_proj_grad, up_proj_grad, down_proj_grad, rows_grad = lax.map(
        expert_pass, (token_rows, grad_rows, gate_proj, up_proj, down_proj))
    picked = rows_grad.reshape(-1, D)[slot_index].reshape(TOKENS, TOP, D)
    token_grad = (cotangent.astype(jnp.float32) + jnp.sum(picked, axis=1)).astype(jnp.bfloat16)

    gate_f32 = gate_in.astype(jnp.float32)
    conv_f32 = conv_in.astype(jnp.float32)
    value_f32 = value_in.astype(jnp.float32)
    product = conv_f32 * value_f32
    padded = jnp.pad(product, ((1, 1), (0, 0)))
    conv_out = conv_taps[0] * padded[:-2] + conv_taps[1] * padded[1:-1] + conv_taps[2] * padded[2:]
    mixed_act = (gate_f32 * conv_out).astype(jnp.bfloat16)
    d_conv_out = jnp.dot(token_grad, out_weight, preferred_element_type=jnp.float32)
    gate_in_grad = (d_conv_out * conv_out).astype(jnp.bfloat16)
    back_signal = d_conv_out * gate_f32
    padded_back = jnp.pad(back_signal, ((1, 1), (0, 0)))
    d_product = conv_taps[0] * padded_back[2:] + conv_taps[1] * padded_back[1:-1] + conv_taps[2] * padded_back[:-2]
    conv_in_grad = (d_product * value_f32).astype(jnp.bfloat16)
    value_in_grad = (d_product * conv_f32).astype(jnp.bfloat16)
    out_weight_grad = jnp.dot(token_grad.T, mixed_act, preferred_element_type=jnp.float32)
    return (gate_proj_grad, up_proj_grad, down_proj_grad, out_weight_grad, token_grad,
            gate_in_grad, conv_in_grad, value_in_grad)
```

```python
import functools
import math

import jax
import jax.numpy as jnp
from jax import lax
from jax.experimental import pallas as pl
from jax.experimental.pallas import tpu as pltpu
from jax.sharding import PartitionSpec as P

CLAMP_LIMIT = 7.0
SILU_ALPHA = 1.702
MESH = pl.DeviceIdType.MESH
BF16 = jnp.bfloat16
F32 = jnp.float32


def dot(left, right, dims):
    return lax.dot_general(left, right, (dims, ((), ())), preferred_element_type=F32)


def rows_dot(left, right):
    return dot(left, right, ((1,), (0,)))


def cols_dot(left, right):
    return dot(left, right, ((1,), (1,)))


def outer_dot(left, right):
    return dot(left, right, ((0,), (0,)))


def neighbours_along(count):
    side = math.isqrt(max(count // 2, 1))
    return side if side and count % side == 0 else 1


def exchange_kernel(
    dims,
    routes_ref, weights_ref, tokens_ref, cot_ref, gate_ref, conv_ref, value_ref, taps_ref,
    outw_hbm, wg_hbm, wu_hbm, wd_hbm,
    x_ref, hid_ref, dg_ref, du_ref, owg_ref, tg_ref, gg_ref, cg_ref, vg_ref,
    tokq, cotq, wg, wu, wd, outw, place, sendb, psend, pown, precv, ysend, yrecv, share, comb,
    tga, prod, halo_p, back, halo_b, conv_s, mixed, feat,
    a_send, a_recv, y_send, y_recv, k_send, k_recv, p_send, p_recv, q_send, q_recv,
    r_send, r_recv, ty_send, ty_recv, tk_send, tk_recv, h_send, h_recv, m_send, m_recv,
    o_send, o_recv, oy_send, oy_recv, ok_send, ok_recv, l_sem,
):
    n_sp, n_tp, nx, cap, quarter, tok, width, chan, fh = dims
    ny = n_tp // 2
    groups = n_sp // nx
    rows = nx * cap
    chunk = width // n_sp
    part = tok // n_tp
    sp, tp = lax.axis_index("sp"), lax.axis_index("tp")
    z, x = sp // nx, sp % nx
    y, c = tp // 2, tp % 2
    partner = (sp, y * 2 + 1 - c)

    def tp_of(yy):
        return yy * 2 + c

    def y_peer(k):
        return (y + k) % ny

    def remote(src, dst, ssem, rsem, dev):
        return pltpu.make_async_remote_copy(
            src_ref=src, dst_ref=dst, send_sem=ssem, recv_sem=rsem,
            device_id=dev, device_id_type=MESH,
        )

    barrier = pltpu.get_barrier_semaphore()

    def greet(n, carry):
        pl.semaphore_signal(barrier, inc=1, device_id=((sp + n) % n_sp, tp), device_id_type=MESH)
        return carry

    lax.fori_loop(1, n_sp, greet, 0)
    for k in range(1, ny):
        pl.semaphore_signal(barrier, inc=1, device_id=(sp, tp_of(y_peer(k))), device_id_type=MESH)
    pl.semaphore_signal(barrier, inc=1, device_id=partner, device_id_type=MESH)

    offset = pl.multiple_of(tp * quarter, quarter)
    loads = [
        pltpu.make_async_copy(tokens_ref.at[:, pl.ds(offset, quarter)], tokq, l_sem.at[0]),
        pltpu.make_async_copy(cot_ref.at[:, pl.ds(offset, quarter)], cotq, l_sem.at[1]),
        pltpu.make_async_copy(wg_hbm.at[0], wg, l_sem.at[2]),
        pltpu.make_async_copy(wu_hbm.at[0], wu, l_sem.at[3]),
        pltpu.make_async_copy(wd_hbm.at[0], wd, l_sem.at[4]),
        pltpu.make_async_copy(outw_hbm, outw, l_sem.at[5]),
    ]
    for load in loads:
        load.start()

    experts = lax.broadcasted_iota(jnp.int32, (n_sp, tok), 0)
    first, second = routes_ref[0:1, :], routes_ref[1:2, :]
    hit_a, hit_b = experts == first, experts == second
    hits = jnp.where(hit_a, 1.0, 0.0) + jnp.where(hit_b, 1.0, 0.0)
    earlier = (
        lax.broadcasted_iota(jnp.int32, (tok, tok), 0) < lax.broadcasted_iota(jnp.int32, (tok, tok), 1)
    )
    before = rows_dot(hits.astype(BF16), jnp.where(earlier, 1.0, 0.0).astype(BF16))

    def slot_of(hit, named):
        rank = jnp.sum(jnp.where(hit, before, 0.0), axis=0, keepdims=True).astype(jnp.int32)
        return named * cap + rank

    slot_a, slot_b = slot_of(hit_a, first), slot_of(hit_b, second)
    weight_a, weight_b = weights_ref[0:1, :], weights_ref[1:2, :]
    slot_iota = lax.broadcasted_iota(jnp.int32, (cap, tok), 0)

    loads[0].wait()
    loads[1].wait()
    pl.semaphore_wait(barrier, (n_sp - 1) + (ny - 1) + 1)

    def dispatch(n, carry):
        d = ((z + n // nx) % groups) * nx + (x + n % nx) % nx
        here_a = slot_iota + d * cap == slot_a
        here_b = slot_iota + d * cap == slot_b
        picked = jnp.where(here_a, 1.0, jnp.where(here_b, 1.0, 0.0)).astype(BF16)
        scale = jnp.sum(
            jnp.where(here_a, weight_a, jnp.where(here_b, weight_b, 0.0)), axis=1, keepdims=True
        )
        place[d] = picked
        sendb[d, 0] = rows_dot(picked, tokq[...]).astype(BF16)
        sendb[d, 1] = (rows_dot(picked, cotq[...]) * scale).astype(BF16)

        @pl.when(d == sp)
        def _():
            x_ref[tp, sp] = sendb[d]

        @pl.when(d != sp)
        def _():
            remote(sendb.at[d], x_ref.at[tp, sp], a_send.at[d], a_recv.at[sp], (d, tp)).start()

        return carry

    lax.fori_loop(0, n_sp, dispatch, 0)

    gate_f = gate_ref[...].astype(F32)
    conv_f = conv_ref[...].astype(F32)
    value_f = value_ref[...].astype(F32)
    prod[...] = conv_f * value_f
    up_dev, down_dev = ((sp + 1) % n_sp, tp), ((sp + n_sp - 1) % n_sp, tp)

    def halo_copies(source, landing, which):
        to_next = remote(
            source.at[pl.ds(tok - 8, 8)], landing.at[0], h_send.at[which, 0], h_recv.at[which, 0], up_dev
        )
        to_prev = remote(
            source.at[pl.ds(0, 8)], landing.at[1], h_send.at[which, 1], h_recv.at[which, 1], down_dev
        )
        return to_next, to_prev

    def halo_start(source, landing, which):
        to_next, to_prev = halo_copies(source, landing, which)

        @pl.when(sp < n_sp - 1)
        def _():
            to_next.start()

        @pl.when(sp == n_sp - 1)
        def _():
            landing[1] = jnp.zeros(landing.shape[1:], F32)

        @pl.when(sp > 0)
        def _():
            to_prev.start()

        @pl.when(sp == 0)
        def _():
            landing[0] = jnp.zeros(landing.shape[1:], F32)

    def halo_finish(source, landing, which):
        to_next, to_prev = halo_copies(source, landing, which)

        @pl.when(sp < n_sp - 1)
        def _():
            to_next.wait_send()
            to_prev.wait_recv()

        @pl.when(sp > 0)
        def _():
            to_prev.wait_send()
            to_next.wait_recv()

    def shifted(cells, landing):
        at_row = lax.broadcasted_iota(jnp.int32, cells.shape, 0)
        above = jnp.where(at_row == 0, landing[0, 7:8, :], pltpu.roll(cells, 1, 0))
        below = jnp.where(at_row == tok - 1, landing[1, 0:1, :], pltpu.roll(cells, tok - 1, 0))
        return above, below

    halo_start(prod, halo_p, 0)
    tap_at = pl.ds(pl.multiple_of(tp * chan, chan), chan)
    tap0, tap1, tap2 = taps_ref[0:1, tap_at], taps_ref[1:2, tap_at], taps_ref[2:3, tap_at]

    def group_of(i):
        return (z + groups - i) % groups

    def arrive(i):
        for j in range(nx):
            s = group_of(i) * nx + (x + nx - j) % nx

            @pl.when(s != sp)
            def _():
                remote(
                    x_ref.at[tp, s], x_ref.at[tp, s], a_send.at[s], a_recv.at[s], (s, tp)
                ).wait_recv()

            for k in range(1, ny):
                yy = y_peer(k)
                remote(
                    x_ref.at[tp, s], x_ref.at[tp, s], y_send.at[yy, s], y_recv.at[y, s], (sp, tp_of(yy))
                ).start()
            remote(
                x_ref.at[tp, s], x_ref.at[tp, s], k_send.at[y, s], k_recv.at[y, s], partner
            ).start()

    def relay(i):
        for j in range(nx):
            s = group_of(i) * nx + (x + nx - j) % nx
            for k in range(1, ny):
                yy = y_peer(k)
                landed = x_ref.at[tp_of(yy), s]
                remote(landed, landed, y_send.at[yy, s], y_recv.at[yy, s], (sp, tp_of(yy))).wait_recv()
                remote(landed, landed, k_send.at[yy, s], k_recv.at[yy, s], partner).start()

    def compute(i):
        g = group_of(i)
        s0 = g * nx
        for j in range(nx):
            for yy in range(ny):
                landed = x_ref.at[yy * 2 + 1 - c, s0 + j]
                remote(landed, landed, k_send.at[yy, s0 + j], k_recv.at[yy, s0 + j], partner).wait_recv()
        gate_pre = jnp.zeros((rows, fh), F32)
        up_pre = jnp.zeros((rows, fh), F32)
        d_hidden = jnp.zeros((rows, fh), F32)
        for q in range(n_tp):
            cells = x_ref[q, pl.ds(s0, nx), 0].reshape(rows, quarter)
            gate_pre += rows_dot(cells, wg[q * quarter:(q + 1) * quarter, :])
            up_pre += rows_dot(cells, wu[q * quarter:(q + 1) * quarter, :])
        for q in range(n_tp):
            cells = x_ref[q, pl.ds(s0, nx), 1].reshape(rows, quarter)
            d_hidden += cols_dot(cells, wd[:, q * quarter:(q + 1) * quarter])
        gate_clip = jnp.minimum(gate_pre, CLAMP_LIMIT)
        up_clip = jnp.clip(up_pre, -CLAMP_LIMIT, CLAMP_LIMIT)
        sig = jax.nn.sigmoid(SILU_ALPHA * gate_clip)
        act = gate_clip * sig
        mine = pl.ds(pl.multiple_of(g * rows, rows), rows)
        hid_ref[mine, :] = ((up_clip + 1.0) * act).astype(BF16)
        d_up = jnp.where(jnp.abs(up_pre) < CLAMP_LIMIT, d_hidden * act, 0.0).astype(BF16)
        slope = sig + SILU_ALPHA * act * (1.0 - sig)
        d_gate = jnp.where(gate_pre < CLAMP_LIMIT, d_hidden * (up_clip + 1.0) * slope, 0.0).astype(BF16)
        dg_ref[mine, :] = d_gate
        du_ref[mine, :] = d_up

        def partial_of(q):
            at = pl.ds(pl.multiple_of(q * quarter, quarter), quarter)
            return cols_dot(d_gate, wg[at, :]) + cols_dot(d_up, wu[at, :])

        for yy in range(ny):
            psend[g, yy] = partial_of(yy * 2 + 1 - c).astype(BF16)
        remote(psend.at[g], precv.at[g], p_send.at[g], p_recv.at[g], partner).start()
        for yy in range(ny):
            pown[g, yy] = partial_of(yy * 2 + c)

    def reduce_cores(i):
        g = group_of(i)
        remote(psend.at[g], precv.at[g], p_send.at[g], p_recv.at[g], partner).wait_recv()
        for k in range(1, ny):
            yy = y_peer(k)
            ysend[g, yy] = (pown[g, yy] + precv[g, yy].astype(F32)).astype(BF16)
            remote(
                ysend.at[g, yy], yrecv.at[g, y], q_send.at[yy, g], q_recv.at[y, g], (sp, tp_of(yy))
            ).start()
        pown[g, y] = pown[g, y] + precv[g, y].astype(F32)

    def give_back(i):
        g = group_of(i)
        total = pown[g, y]
        for k in range(1, ny):
            yy = y_peer(k)
            remote(
                ysend.at[g, yy], yrecv.at[g, yy], q_send.at[yy, g], q_recv.at[yy, g], (sp, tp_of(yy))
            ).wait_recv()
            total = total + yrecv[g, yy].astype(F32)
        share[pl.ds(g * nx, nx)] = total.astype(BF16).reshape(nx, cap, quarter)
        for j in range(nx):
            s = g * nx + (x + j) % nx

            @pl.when(s != sp)
            def _():
                remote(share.at[s], comb.at[sp], r_send.at[s], r_recv.at[sp], (s, tp)).start()

            @pl.when(s == sp)
            def _():
                comb[s] = share[s]

    for load in loads[2:]:
        load.wait()

    def step(i, carry):
        pl.when(i < groups)(lambda: arrive(i))
        pl.when((i >= 2) & (i < groups + 2))(lambda: compute(i - 2))
        pl.when((i >= 1) & (i < groups + 1))(lambda: relay(i - 1))
        pl.when((i >= 2) & (i < groups + 2))(lambda: reduce_cores(i - 2))
        pl.when(i >= 3)(lambda: give_back(i - 3))
        return carry

    lax.fori_loop(0, groups + 3, step, 0)

    halo_finish(prod, halo_p, 0)
    above, below = shifted(prod[...], halo_p)
    conv_out = tap0 * above + tap1 * prod[...] + tap2 * below
    conv_s[...] = conv_out
    mixed[sp] = (gate_f * conv_out).astype(BF16)

    def send_mixed(n, carry):
        d = (sp + n) % n_sp
        remote(mixed.at[sp], mixed.at[sp], m_send.at[d], m_recv.at[sp], (d, tp)).start()
        return carry

    lax.fori_loop(1, n_sp, send_mixed, 0)

    tg_ref[...] = jnp.zeros_like(tg_ref)

    def collect(n, acc):
        d = ((z + n // nx) % groups) * nx + (x + n % nx) % nx

        @pl.when(d != sp)
        def _():
            remote(share.at[d], comb.at[d], r_send.at[d], r_recv.at[d], (d, tp)).wait_recv()

        return acc + outer_dot(place[d], comb[d])

    acc = lax.fori_loop(0, n_sp, collect, cotq[...].astype(F32))
    token_grad = acc.astype(BF16)
    tg_ref[...] = token_grad
    tga[tp] = token_grad

    for k in range(1, ny):
        yy = y_peer(k)
        remote(tga.at[tp], tga.at[tp], ty_send.at[yy], ty_recv.at[y], (sp, tp_of(yy))).start()
    remote(tga.at[tp], tga.at[tp], tk_send.at[y], tk_recv.at[y], partner).start()
    for k in range(1, ny):
        yy = y_peer(k)
        landed = tga.at[tp_of(yy)]
        remote(landed, landed, ty_send.at[yy], ty_recv.at[yy], (sp, tp_of(yy))).wait_recv()
        remote(landed, landed, tk_send.at[yy], tk_recv.at[yy], partner).start()
    for yy in range(ny):
        landed = tga.at[yy * 2 + 1 - c]
        remote(landed, landed, tk_send.at[yy], tk_recv.at[yy], partner).wait_recv()

    def feature_of(d):
        lane = (d * chunk) % quarter
        return tga.at[
            (d * chunk) // quarter,
            pl.ds(pl.multiple_of(tp * part, part), part),
            pl.ds(pl.multiple_of(lane, chunk), chunk),
        ]

    def send_features(n, carry):
        d = (sp + n) % n_sp
        remote(feature_of(d), feat.at[tp, sp], o_send.at[d], o_recv.at[sp], (d, tp)).start()
        return carry

    lax.fori_loop(1, n_sp, send_features, 0)
    feat[tp, sp] = feature_of(sp)[...]

    d_conv = jnp.zeros((tok, chan), F32)
    for q in range(n_tp):
        d_conv += rows_dot(tga[q], outw[q * quarter:(q + 1) * quarter, :])
    back[...] = d_conv * gate_f
    halo_start(back, halo_b, 1)
    gg_ref[...] = (d_conv * conv_s[...]).astype(BF16)

    halo_finish(back, halo_b, 1)
    above, below = shifted(back[...], halo_b)
    d_prod = tap0 * below + tap1 * back[...] + tap2 * above
    cg_ref[...] = (d_prod * value_f).astype(BF16)
    vg_ref[...] = (d_prod * conv_f).astype(BF16)

    def land_features(n, carry):
        s = (sp + n_sp - n) % n_sp
        landed = feat.at[tp, s]
        remote(feature_of(s), landed, o_send.at[s], o_recv.at[s], (s, tp)).wait_recv()
        return carry

    lax.fori_loop(1, n_sp, land_features, 0)
    for k in range(1, ny):
        yy = y_peer(k)
        remote(feat.at[tp], feat.at[tp], oy_send.at[yy], oy_recv.at[y], (sp, tp_of(yy))).start()
    remote(feat.at[tp], feat.at[tp], ok_send.at[y], ok_recv.at[y], partner).start()

    def land_mixed(n, carry):
        s = (sp + n_sp - n) % n_sp
        remote(mixed.at[s], mixed.at[s], m_send.at[s], m_recv.at[s], (s, tp)).wait_recv()
        return carry

    lax.fori_loop(1, n_sp, land_mixed, 0)
    for k in range(1, ny):
        yy = y_peer(k)
        landed = feat.at[tp_of(yy)]
        remote(landed, landed, oy_send.at[yy], oy_recv.at[yy], (sp, tp_of(yy))).wait_recv()
        remote(landed, landed, ok_send.at[yy], ok_recv.at[yy], partner).start()
    for yy in range(ny):
        landed = feat.at[yy * 2 + 1 - c]
        remote(landed, landed, ok_send.at[yy], ok_recv.at[yy], partner).wait_recv()
    owg = jnp.zeros((chunk, chan), F32)
    for t in range(n_tp):
        left = feat[t].reshape(n_sp * part, chunk)
        right = mixed[:, t * part:(t + 1) * part, :].reshape(n_sp * part, chan)
        owg += outer_dot(left, right)
    owg_ref[...] = owg

    def drain(n, carry):
        d = (sp + n) % n_sp
        remote(sendb.at[d], sendb.at[d], a_send.at[d], a_recv.at[d], (d, tp)).wait_send()
        remote(share.at[d], share.at[d], r_send.at[d], r_recv.at[d], (d, tp)).wait_send()
        remote(mixed.at[sp], mixed.at[sp], m_send.at[d], m_recv.at[d], (d, tp)).wait_send()
        remote(feature_of(d), feat.at[tp, sp], o_send.at[d], o_recv.at[d], (d, tp)).wait_send()
        return carry

    lax.fori_loop(1, n_sp, drain, 0)

    def drain_blocks(s, carry):
        for k in range(1, ny):
            yy = y_peer(k)
            mine = x_ref.at[tp, s]
            remote(mine, mine, y_send.at[yy, s], y_recv.at[yy, s], (sp, tp_of(yy))).wait_send()
        for yy in range(ny):
            mine = x_ref.at[tp_of(yy), s]
            remote(mine, mine, k_send.at[yy, s], k_recv.at[yy, s], partner).wait_send()
        return carry

    lax.fori_loop(0, n_sp, drain_blocks, 0)

    def drain_groups(g, carry):
        remote(psend.at[g], precv.at[g], p_send.at[g], p_recv.at[g], partner).wait_send()
        for k in range(1, ny):
            yy = y_peer(k)
            remote(
                ysend.at[g, yy], yrecv.at[g, y], q_send.at[yy, g], q_recv.at[y, g], (sp, tp_of(yy))
            ).wait_send()
        return carry

    lax.fori_loop(0, groups, drain_groups, 0)
    for k in range(1, ny):
        yy = y_peer(k)
        remote(tga.at[tp], tga.at[tp], ty_send.at[yy], ty_recv.at[y], (sp, tp_of(yy))).wait_send()
        remote(feat.at[tp], feat.at[tp], oy_send.at[yy], oy_recv.at[y], (sp, tp_of(yy))).wait_send()
    for yy in range(ny):
        mine = tga.at[tp_of(yy)]
        remote(mine, mine, tk_send.at[yy], tk_recv.at[yy], partner).wait_send()
        mine = feat.at[tp_of(yy)]
        remote(mine, mine, ok_send.at[yy], ok_recv.at[yy], partner).wait_send()


def grads_kernel(
    x_ref, hid_ref, dg_ref, du_ref, owg_in, tg_in, gg_in, cg_in, vg_in,
    gate_out, up_out, down_out, owg_out, tg_out, gg_out, cg_out, vg_out, hid_t,
):
    slots = hid_ref.shape[0]
    quarter = x_ref.shape[-1]

    @pl.when(pl.program_id(0) == 0)
    def _():
        hid_t[...] = hid_ref[...].T
        owg_out[...] = owg_in[...]
        tg_out[...] = tg_in[...]
        gg_out[...] = gg_in[...]
        cg_out[...] = cg_in[...]
        vg_out[...] = vg_in[...]

    rows = x_ref[0, :, 0].reshape(slots, quarter).T
    grads = x_ref[0, :, 1].reshape(slots, quarter)
    gate_out[0] = rows_dot(rows, dg_ref[...])
    up_out[0] = rows_dot(rows, du_ref[...])
    down_out[0] = rows_dot(hid_t[...], grads)


def local_kernels(
    saved_tokens, cotangent, routes, route_weights, gate_in, conv_in, value_in, conv_taps,
    out_weight, gate_proj, up_proj, down_proj,
):
    tok, width = saved_tokens.shape
    n_sp, n_tp = lax.axis_size("sp"), lax.axis_size("tp")
    top = routes.shape[1]
    cap = 2 * tok * top // n_sp
    nx = neighbours_along(n_sp)
    ny, groups = n_tp // 2, n_sp // nx
    quarter = width // n_tp
    chan = gate_in.shape[1]
    fh = gate_proj.shape[2]
    chunk, part = width // n_sp, tok // n_tp
    rows = nx * cap
    slots = n_sp * cap
    dims = (n_sp, n_tp, nx, cap, quarter, tok, width, chan, fh)
    vmem = pl.BlockSpec(memory_space=pltpu.VMEM)
    hbm = pl.BlockSpec(memory_space=pl.ANY)
    dma = pltpu.SemaphoreType.DMA
    struct = jax.ShapeDtypeStruct
    outs = pl.pallas_call(
        functools.partial(exchange_kernel, dims),
        name="exchange",
        out_shape=(
            struct((n_tp, n_sp, 2, cap, quarter), BF16),
            struct((slots, fh), BF16),
            struct((slots, fh), BF16),
            struct((slots, fh), BF16),
            struct((chunk, chan), F32),
            struct((tok, quarter), BF16),
            struct((tok, chan), BF16),
            struct((tok, chan), BF16),
            struct((tok, chan), BF16),
        ),
        in_specs=[vmem, vmem, hbm, hbm, vmem, vmem, vmem, vmem, hbm, hbm, hbm, hbm],
        out_specs=(vmem,) * 9,
        scratch_shapes=[
            pltpu.VMEM((tok, quarter), BF16),
            pltpu.VMEM((tok, quarter), BF16),
            pltpu.VMEM((width, fh), BF16),
            pltpu.VMEM((width, fh), BF16),
            pltpu.VMEM((fh, width), BF16),
            pltpu.VMEM((width, chan), BF16),
            pltpu.VMEM((n_sp, cap, tok), BF16),
            pltpu.VMEM((n_sp, 2, cap, quarter), BF16),
            pltpu.VMEM((groups, ny, rows, quarter), BF16),
            pltpu.VMEM((groups, ny, rows, quarter), F32),
            pltpu.VMEM((groups, ny, rows, quarter), BF16),
            pltpu.VMEM((groups, ny, rows, quarter), BF16),
            pltpu.VMEM((groups, ny, rows, quarter), BF16),
            pltpu.VMEM((n_sp, cap, quarter), BF16),
            pltpu.VMEM((n_sp, cap, quarter), BF16),
            pltpu.VMEM((n_tp, tok, quarter), BF16),
            pltpu.VMEM((tok, chan), F32),
            pltpu.VMEM((2, 8, chan), F32),
            pltpu.VMEM((tok, chan), F32),
            pltpu.VMEM((2, 8, chan), F32),
            pltpu.VMEM((tok, chan), F32),
            pltpu.VMEM((n_sp, tok, chan), BF16),
            pltpu.VMEM((n_tp, n_sp, part, chunk), BF16),
            dma((n_sp,)), dma((n_sp,)),
            dma((ny, n_sp)), dma((ny, n_sp)),
            dma((ny, n_sp)), dma((ny, n_sp)),
            dma((groups,)), dma((groups,)),
            dma((ny, groups)), dma((ny, groups)),
            dma((n_sp,)), dma((n_sp,)),
            dma((ny,)), dma((ny,)),
            dma((ny,)), dma((ny,)),
            dma((2, 2)), dma((2, 2)),
            dma((n_sp,)), dma((n_sp,)),
            dma((n_sp,)), dma((n_sp,)),
            dma((ny,)), dma((ny,)),
            dma((ny,)), dma((ny,)),
            dma((6,)),
        ],
        compiler_params=pltpu.CompilerParams(collective_id=0, has_side_effects=True),
    )(
        routes.T, route_weights.T, saved_tokens, cotangent, gate_in, conv_in, value_in, conv_taps,
        out_weight, gate_proj, up_proj, down_proj,
    )
    exchanged, small = outs[:4], outs[4:]
    whole = [pl.BlockSpec(a.shape, lambda q, n=a.ndim: (0,) * n) for a in exchanged[1:]]
    passed = [pl.BlockSpec(a.shape, lambda q, n=a.ndim: (0,) * n) for a in small]
    return pl.pallas_call(
        grads_kernel,
        name="weight_grads",
        grid=(n_tp,),
        out_shape=(
            struct((1, width, fh), F32),
            struct((1, width, fh), F32),
            struct((1, fh, width), F32),
        ) + tuple(struct(a.shape, a.dtype) for a in small),
        in_specs=[pl.BlockSpec((1,) + exchanged[0].shape[1:], lambda q: (q, 0, 0, 0, 0))] + whole + passed,
        out_specs=[
            pl.BlockSpec((1, quarter, fh), lambda q: (0, q, 0)),
            pl.BlockSpec((1, quarter, fh), lambda q: (0, q, 0)),
            pl.BlockSpec((1, fh, quarter), lambda q: (0, 0, q)),
        ] + passed,
        scratch_shapes=[pltpu.VMEM((fh, slots), BF16)],
    )(*exchanged, *small)


def contract_rows(left, right):
    return lax.dot_general(
        left, right, (((0,), (0,)), ((), ())), preferred_element_type=jnp.float32
    )


def contract_cols(left, right):
    return lax.dot_general(
        left, right, (((1,), (1,)), ((), ())), preferred_element_type=jnp.float32
    )


def halo(cells, axis):
    count = lax.axis_size(axis)
    ends = count - 1
    above = lax.ppermute(cells[-1:], axis, [(i, (i + 1) % count) for i in range(ends)])
    below = lax.ppermute(cells[:1], axis, [((i + 1) % count, i) for i in range(ends)])
    return jnp.concatenate([above, cells, below], axis=0)


def exchange_groups(partial_value, part_width):
    tp_count = lax.axis_size("tp")
    pairs = tp_count // 2
    me = lax.axis_index("tp")
    side, pair = me % 2, me // 2

    def block(which_pair, which_side):
        return lax.dynamic_slice_in_dim(
            partial_value, (2 * which_pair + which_side) * part_width, part_width, 1
        )

    others = [(i, i ^ 1) for i in range(tp_count)]
    sums = []
    for step in range(1, pairs + 1):
        target = (pair + step) % pairs
        given = block(target, 1 - side).astype(jnp.bfloat16)
        got = lax.ppermute(given, "tp", others)
        sums.append(block(target, side) + got.astype(jnp.float32))
    total = sums[-1]
    for step in range(1, pairs):
        moves = [(i, (i + 2 * step) % tp_count) for i in range(tp_count)]
        got = lax.ppermute(sums[step - 1].astype(jnp.bfloat16), "tp", moves)
        total = total + got.astype(jnp.float32)
    return total


def gather_features(part):
    tp_count = lax.axis_size("tp")
    pairs = tp_count // 2
    me = lax.axis_index("tp")
    side, pair = me % 2, me // 2
    width = part.shape[1]
    others = [(i, i ^ 1) for i in range(tp_count)]
    held = [part]
    for step in range(1, pairs):
        moves = [(i, (i + 2 * step) % tp_count) for i in range(tp_count)]
        held.append(lax.ppermute(part, "tp", moves))
    twins = [lax.ppermute(block, "tp", others) for block in held]
    whole = jnp.zeros((part.shape[0], tp_count * width), part.dtype)
    for step in range(pairs):
        first = 2 * ((pair - step) % pairs)
        whole = lax.dynamic_update_slice_in_dim(whole, held[step], (first + side) * width, 1)
        whole = lax.dynamic_update_slice_in_dim(whole, twins[step], (first + 1 - side) * width, 1)
    return whole


def local_collectives(
    saved_tokens,
    cotangent,
    routes,
    route_weights,
    gate_in,
    conv_in,
    value_in,
    conv_taps,
    out_weight,
    gate_proj,
    up_proj,
    down_proj,
):
    tok_rows, model_width = saved_tokens.shape
    top_count = routes.shape[1]
    expert_count = lax.axis_size("sp")
    tp_count = lax.axis_size("tp")
    capacity = 2 * tok_rows * top_count // expert_count
    slots = expert_count * capacity
    part_width = model_width // tp_count
    channels = gate_in.shape[1]
    me_tp = lax.axis_index("tp")
    offset = me_tp * part_width

    routes_t = routes.T
    weights_t = route_weights.T
    experts = lax.broadcasted_iota(jnp.int32, (expert_count, tok_rows), 0)
    chosen = [experts == routes_t[k][None, :] for k in range(top_count)]
    hits = sum(c.astype(jnp.bfloat16) for c in chosen)
    earlier = (
        lax.broadcasted_iota(jnp.int32, (tok_rows, tok_rows), 0)
        < lax.broadcasted_iota(jnp.int32, (tok_rows, tok_rows), 1)
    ).astype(jnp.bfloat16)
    before = jnp.dot(hits, earlier, preferred_element_type=jnp.float32)
    slot_ids = lax.broadcasted_iota(jnp.int32, (slots, tok_rows), 0)
    place = jnp.zeros((slots, tok_rows), jnp.float32)
    weighted = jnp.zeros((slots, tok_rows), jnp.float32)
    for k in range(top_count):
        rank = jnp.sum(jnp.where(chosen[k], before, 0.0), axis=0).astype(jnp.int32)
        here = slot_ids == (routes_t[k] * capacity + rank)[None, :]
        place = jnp.where(here, 1.0, place)
        weighted = jnp.where(here, weights_t[k][None, :], weighted)
    place = place.astype(jnp.bfloat16)
    slot_weight = jnp.sum(weighted, axis=1, keepdims=True)

    own_tokens = lax.dynamic_slice_in_dim(saved_tokens, offset, part_width, 1)
    own_cot = lax.dynamic_slice_in_dim(cotangent, offset, part_width, 1)
    send_tokens = jnp.dot(place, own_tokens, preferred_element_type=jnp.float32).astype(jnp.bfloat16)
    cot_rows = jnp.dot(place, own_cot, preferred_element_type=jnp.float32)
    send_grads = (cot_rows * slot_weight).astype(jnp.bfloat16)

    def dispatched(rows):
        rows = rows.reshape(expert_count, capacity, part_width)
        return lax.all_to_all(rows, "sp", split_axis=0, concat_axis=0, tiled=True)

    arrived_tokens = dispatched(send_tokens)
    arrived_tokens, send_grads = lax.optimization_barrier((arrived_tokens, send_grads))
    arrived_grads = dispatched(send_grads)
    rows_in = gather_features(arrived_tokens.reshape(slots, part_width))
    grads_in = gather_features(arrived_grads.reshape(slots, part_width))

    gate_f32 = gate_in.astype(jnp.float32)
    conv_f32 = conv_in.astype(jnp.float32)
    value_f32 = value_in.astype(jnp.float32)
    my_taps = lax.dynamic_slice_in_dim(conv_taps, me_tp * channels, channels, 1)
    prod_rim = halo(conv_f32 * value_f32, "sp")
    conv_out = my_taps[0] * prod_rim[:-2] + my_taps[1] * prod_rim[1:-1] + my_taps[2] * prod_rim[2:]
    mixed = (gate_f32 * conv_out).astype(jnp.bfloat16)
    mixed = jnp.concatenate([mixed, mixed], axis=1)

    w_gate, w_up, w_down = gate_proj[0], up_proj[0], down_proj[0]
    gate_pre = jnp.dot(rows_in, w_gate, preferred_element_type=jnp.float32)
    up_pre = jnp.dot(rows_in, w_up, preferred_element_type=jnp.float32)
    gate_clip = jnp.minimum(gate_pre, CLAMP_LIMIT)
    up_clip = jnp.clip(up_pre, -CLAMP_LIMIT, CLAMP_LIMIT)
    sigmoid_gate = jax.nn.sigmoid(SILU_ALPHA * gate_clip)
    gated_act = gate_clip * sigmoid_gate
    hidden = ((up_clip + 1.0) * gated_act).astype(jnp.bfloat16)
    grads_in, mixed = lax.optimization_barrier((grads_in, mixed))
    mixed_all = lax.all_gather(mixed, "sp", axis=0, tiled=True)
    d_hidden = contract_cols(grads_in, w_down)
    d_up = jnp.where(jnp.abs(up_pre) < CLAMP_LIMIT, d_hidden * gated_act, 0.0).astype(jnp.bfloat16)
    gate_slope = sigmoid_gate + SILU_ALPHA * gate_clip * sigmoid_gate * (1.0 - sigmoid_gate)
    d_gate = jnp.where(gate_pre < CLAMP_LIMIT, d_hidden * (up_clip + 1.0) * gate_slope, 0.0).astype(
        jnp.bfloat16
    )
    partial_value = contract_cols(d_gate, w_gate) + contract_cols(d_up, w_up)
    shares = exchange_groups(partial_value, part_width).astype(jnp.bfloat16)
    down_grad = contract_rows(hidden, grads_in)
    gate_grad = contract_rows(rows_in, d_gate)
    up_grad = contract_rows(rows_in, d_up)

    returned = dispatched(shares).reshape(slots, part_width)
    combined = contract_rows(place, returned)
    token_grad = (own_cot.astype(jnp.float32) + combined).astype(jnp.bfloat16)
    residual = lax.all_gather(token_grad, "tp", axis=1, tiled=True)

    d_conv_out = jnp.dot(residual, out_weight, preferred_element_type=jnp.float32)
    grad_rim = halo(d_conv_out * gate_f32, "sp")
    d_product = my_taps[0] * grad_rim[2:] + my_taps[1] * grad_rim[1:-1] + my_taps[2] * grad_rim[:-2]
    gate_in_grad = (d_conv_out * conv_out).astype(jnp.bfloat16)
    conv_in_grad = (d_product * value_f32).astype(jnp.bfloat16)
    value_in_grad = (d_product * conv_f32).astype(jnp.bfloat16)

    share = tok_rows // tp_count
    quarter = lax.dynamic_slice_in_dim(residual, me_tp * share, share, 0)
    quarter = quarter.reshape(share, expert_count, model_width // expert_count)
    quarter = lax.all_to_all(
        quarter.transpose(1, 0, 2), "sp", split_axis=0, concat_axis=0, tiled=True
    )
    features = lax.all_gather(quarter, "tp", axis=1, tiled=True)
    features = features.reshape(expert_count * tok_rows, -1)
    out_weight_grad = contract_rows(features, mixed_all[:, :channels])
    return (
        gate_grad[None],
        up_grad[None],
        down_grad[None],
        out_weight_grad,
        token_grad,
        gate_in_grad,
        conv_in_grad,
        value_in_grad,
    )


def local(*arrays):
    tok, width = arrays[0].shape
    n_sp, n_tp = lax.axis_size("sp"), lax.axis_size("tp")
    cap = 2 * tok * arrays[2].shape[1] // n_sp
    aligned = (
        arrays[2].shape[1] == 2
        and n_tp % 2 == 0
        and cap % 16 == 0
        and tok % (16 * n_tp) == 0
        and width % (128 * n_sp) == 0
        and (width // n_tp) % (width // n_sp) == 0
    )
    return (local_kernels if aligned else local_collectives)(*arrays)


def solution(mesh):
    in_specs = (
        P("sp", None),
        P("sp", None),
        P("sp", None),
        P("sp", None),
        P("sp", "tp"),
        P("sp", "tp"),
        P("sp", "tp"),
        P(),
        P(None, "tp"),
        P("sp", None, "tp"),
        P("sp", None, "tp"),
        P("sp", "tp", None),
    )
    out_specs = (
        P("sp", None, "tp"),
        P("sp", None, "tp"),
        P("sp", "tp", None),
        P("sp", "tp"),
        P("sp", "tp"),
        P("sp", "tp"),
        P("sp", "tp"),
        P("sp", "tp"),
    )
    return jax.shard_map(local, mesh=mesh, in_specs=in_specs, out_specs=out_specs, check_vma=False)
```

```python
import functools

import jax
import jax.numpy as jnp
from jax import lax
from jax.experimental import pallas as pl
from jax.experimental.pallas import tpu as pltpu
from jax.sharding import PartitionSpec as P

CLAMP_LIMIT = 7.0
SILU_ALPHA = 1.702
AHEAD = 2
MESH = pl.DeviceIdType.MESH
BF16 = jnp.bfloat16
F32 = jnp.float32


def dot(left, right, dims):
    return lax.dot_general(left, right, (dims, ((), ())), preferred_element_type=F32)


def rows_dot(left, right):
    return dot(left, right, ((1,), (0,)))


def cols_dot(left, right):
    return dot(left, right, ((1,), (1,)))


def outer_dot(left, right):
    return dot(left, right, ((0,), (0,)))


def exchange_kernel(
    dims,
    routes_hbm, weights_hbm, tokens_hbm, cot_hbm, gate_hbm, conv_hbm, value_hbm, taps_hbm,
    outw_hbm, wg_hbm, wu_hbm, wd_hbm,
    gate_out, up_out, down_out, owg_ref, tg_ref, gg_ref, cg_ref, vg_ref,
    x_ref, hid_ref, dg_ref, du_ref, hid_t,
    routes_ref, weights_ref, tokens_ref, cot_ref, gate_ref, conv_ref, value_ref, taps_ref,
    wg, wu, wd, outw, place, sendb, psend, pown, precv, ysend, yrecv, share, comb,
    tga, prod, halo_p, back, halo_b, conv_s, mixed, feat,
    a_send, a_recv, y_send, y_recv, k_send, k_recv, p_send, p_recv, q_send, q_recv,
    r_send, r_recv, ty_send, ty_recv, tk_send, tk_recv, h_send, h_recv, m_send, m_recv,
    o_send, o_recv, ok_send, ok_recv, l_sem,
):
    n_sp, n_tp, cap, quarter, tok, width, chan, fh = dims
    ny = n_tp // 2
    half = n_sp // 2
    slots = n_sp * cap
    chunk = width // n_sp
    part = tok // 2
    sp, tp = lax.axis_index("sp"), lax.axis_index("tp")
    side, pos = sp // half, sp % half
    mirror = (1 - side) * half + pos
    y, c = tp // 2, tp % 2
    partner = (sp, y * 2 + 1 - c)

    def near(r):
        return side * half + (pos + half + r) % half

    def far(r):
        return (1 - side) * half + (pos + half + r) % half

    def tp_of(yy):
        return yy * 2 + c

    def y_peer(k):
        return (y + k) % ny

    def remote(src, dst, ssem, rsem, dev):
        return pltpu.make_async_remote_copy(
            src_ref=src, dst_ref=dst, send_sem=ssem, recv_sem=rsem,
            device_id=dev, device_id_type=MESH,
        )

    barrier = pltpu.get_barrier_semaphore()

    def greet(n, carry):
        pl.semaphore_signal(barrier, inc=1, device_id=((sp + n) % n_sp, tp), device_id_type=MESH)
        return carry

    lax.fori_loop(1, n_sp, greet, 0)
    for k in range(1, ny):
        pl.semaphore_signal(barrier, inc=1, device_id=(sp, tp_of(y_peer(k))), device_id_type=MESH)
    pl.semaphore_signal(barrier, inc=1, device_id=partner, device_id_type=MESH)

    sources = (
        routes_hbm, weights_hbm, tokens_hbm, cot_hbm, gate_hbm, conv_hbm, value_hbm, taps_hbm,
        wg_hbm.at[0], wu_hbm.at[0], wd_hbm.at[0], outw_hbm,
    )
    targets = (
        routes_ref, weights_ref, tokens_ref, cot_ref, gate_ref, conv_ref, value_ref, taps_ref,
        wg, wu, wd, outw,
    )
    loads = [
        pltpu.make_async_copy(source, target, l_sem.at[n])
        for n, (source, target) in enumerate(zip(sources, targets))
    ]
    early, late = loads[2:8], loads[8:]
    for load in loads:
        load.start()

    loads[0].wait()
    loads[1].wait()
    experts = lax.broadcasted_iota(jnp.int32, (n_sp, tok), 0)
    first, second = routes_ref[0:1, :], routes_ref[1:2, :]
    hit_a, hit_b = experts == first, experts == second
    hits = jnp.where(hit_a, 1.0, 0.0) + jnp.where(hit_b, 1.0, 0.0)
    earlier = (
        lax.broadcasted_iota(jnp.int32, (tok, tok), 0) < lax.broadcasted_iota(jnp.int32, (tok, tok), 1)
    )
    before = rows_dot(hits.astype(BF16), jnp.where(earlier, 1.0, 0.0).astype(BF16))

    def slot_of(hit, named):
        rank = jnp.sum(jnp.where(hit, before, 0.0), axis=0, keepdims=True).astype(jnp.int32)
        return named * cap + rank

    slot_a, slot_b = slot_of(hit_a, first), slot_of(hit_b, second)
    weight_a, weight_b = weights_ref[0:1, :], weights_ref[1:2, :]
    slot_iota = lax.broadcasted_iota(jnp.int32, (cap, tok), 0)
    own = pl.ds(pl.multiple_of(tp * quarter, quarter), quarter)

    def placed(d):
        here_a = slot_iota + d * cap == slot_a
        here_b = slot_iota + d * cap == slot_b
        picked = jnp.where(here_a, 1.0, jnp.where(here_b, 1.0, 0.0)).astype(BF16)
        scale = jnp.sum(
            jnp.where(here_a, weight_a, jnp.where(here_b, weight_b, 0.0)), axis=1, keepdims=True
        )
        place[d] = picked
        return picked, scale

    def send_block(d):
        picked, scale = placed(d)
        sendb[d, 0] = rows_dot(picked, tokens_ref[:, own]).astype(BF16)
        sendb[d, 1] = (rows_dot(picked, cot_ref[:, own]) * scale).astype(BF16)
        remote(sendb.at[d], x_ref.at[tp, sp], a_send.at[d], a_recv.at[sp], (d, tp)).start()

    for load in early:
        load.wait()
    gate_f = gate_ref[...].astype(F32)
    conv_f = conv_ref[...].astype(F32)
    value_f = value_ref[...].astype(F32)
    prod[...] = conv_f * value_f
    up_dev, down_dev = ((sp + 1) % n_sp, tp), ((sp + n_sp - 1) % n_sp, tp)

    def halo_copies(source, landing, which):
        to_next = remote(
            source.at[pl.ds(tok - 8, 8)], landing.at[0], h_send.at[which, 0], h_recv.at[which, 0], up_dev
        )
        to_prev = remote(
            source.at[pl.ds(0, 8)], landing.at[1], h_send.at[which, 1], h_recv.at[which, 1], down_dev
        )
        return to_next, to_prev

    def halo_start(source, landing, which):
        to_next, to_prev = halo_copies(source, landing, which)

        @pl.when(sp < n_sp - 1)
        def _():
            to_next.start()

        @pl.when(sp == n_sp - 1)
        def _():
            landing[1] = jnp.zeros(landing.shape[1:], F32)

        @pl.when(sp > 0)
        def _():
            to_prev.start()

        @pl.when(sp == 0)
        def _():
            landing[0] = jnp.zeros(landing.shape[1:], F32)

    def halo_finish(source, landing, which):
        to_next, to_prev = halo_copies(source, landing, which)

        @pl.when(sp < n_sp - 1)
        def _():
            to_next.wait_send()
            to_prev.wait_recv()

        @pl.when(sp > 0)
        def _():
            to_prev.wait_send()
            to_next.wait_recv()

    def shifted(cells, landing):
        at_row = lax.broadcasted_iota(jnp.int32, cells.shape, 0)
        above = jnp.where(at_row == 0, landing[0, 7:8, :], pltpu.roll(cells, 1, 0))
        below = jnp.where(at_row == tok - 1, landing[1, 0:1, :], pltpu.roll(cells, tok - 1, 0))
        return above, below

    pl.semaphore_wait(barrier, (n_sp - 1) + (ny - 1) + 1)
    halo_start(prod, halo_p, 0)
    tap_at = pl.ds(pl.multiple_of(tp * chan, chan), chan)
    tap0, tap1, tap2 = taps_ref[0:1, tap_at], taps_ref[1:2, tap_at], taps_ref[2:3, tap_at]


    def dispatch(r):
        send_block(far(r))
        pl.when(r + 1 < half)(lambda: send_block(near(r + 1)))

    def dispatched(r):
        d = far(r)
        remote(sendb.at[d], sendb.at[d], a_send.at[d], a_recv.at[d], (d, tp)).wait_send()

    for r in range(min(AHEAD, half)):
        dispatch(r)

    picked, scale = placed(sp)
    for q in range(n_tp):
        at = slice(q * quarter, (q + 1) * quarter)
        x_ref[q, sp, 0] = rows_dot(picked, tokens_ref[:, at]).astype(BF16)
        x_ref[q, sp, 1] = (rows_dot(picked, cot_ref[:, at]) * scale).astype(BF16)

    halo_finish(prod, halo_p, 0)
    above, below = shifted(prod[...], halo_p)
    conv_out = tap0 * above + tap1 * prod[...] + tap2 * below
    conv_s[...] = conv_out
    mixed[sp] = (gate_f * conv_out).astype(BF16)

    def mixed_copy(b, which, d):
        return remote(mixed.at[b], mixed.at[b], m_send.at[which, d], m_recv.at[b], (d, tp))

    mixed_copy(sp, 0, mirror).start()

    def spread_own(r, carry):
        mixed_copy(sp, 0, near(r)).start()
        return carry

    lax.fori_loop(1, half, spread_own, 0)

    def spread_mirror():
        mixed_copy(mirror, 0, mirror).wait_recv()

        def one(r, carry):
            mixed_copy(mirror, 1, near(r)).start()
            return carry

        lax.fori_loop(1, half, one, 0)

    def land(s):
        landed = x_ref.at[tp, s]
        remote(landed, landed, a_send.at[s], a_recv.at[s], (s, tp)).wait_recv()
        for k in range(1, ny):
            yy = y_peer(k)
            remote(landed, landed, y_send.at[yy, s], y_recv.at[y, s], (sp, tp_of(yy))).start()
        remote(landed, landed, k_send.at[y, s], k_recv.at[y, s], partner).start()

    def arrive(i):
        dispatched(i)
        pl.when(i + AHEAD < half)(lambda: dispatch(i + AHEAD))
        pl.when(i + 1 < half)(lambda: land(near(-i - 1)))
        land(far(-i))

    def pass_on(s):
        for k in range(1, ny):
            yy = y_peer(k)
            landed = x_ref.at[tp_of(yy), s]
            remote(landed, landed, y_send.at[yy, s], y_recv.at[yy, s], (sp, tp_of(yy))).wait_recv()
            remote(landed, landed, k_send.at[yy, s], k_recv.at[yy, s], partner).start()

    def relay(i):
        pl.when(i + 1 < half)(lambda: pass_on(near(-i - 1)))
        pass_on(far(-i))

    def complete(s):
        for yy in range(ny):
            landed = x_ref.at[yy * 2 + 1 - c, s]
            remote(landed, landed, k_send.at[yy, s], k_recv.at[yy, s], partner).wait_recv()

    def compute(i):
        blocks = (near(-i), far(-i))
        pl.when(i > 0)(lambda: complete(blocks[0]))
        complete(blocks[1])

        def cells(q, which):
            return jnp.concatenate([x_ref[q, s, which] for s in blocks], axis=0)

        rows = 2 * cap
        gate_pre = jnp.zeros((rows, fh), F32)
        up_pre = jnp.zeros((rows, fh), F32)
        d_hidden = jnp.zeros((rows, fh), F32)
        for q in range(n_tp):
            gate_pre += rows_dot(cells(q, 0), wg[q * quarter:(q + 1) * quarter, :])
            up_pre += rows_dot(cells(q, 0), wu[q * quarter:(q + 1) * quarter, :])
        for q in range(n_tp):
            d_hidden += cols_dot(cells(q, 1), wd[:, q * quarter:(q + 1) * quarter])
        gate_clip = jnp.minimum(gate_pre, CLAMP_LIMIT)
        up_clip = jnp.clip(up_pre, -CLAMP_LIMIT, CLAMP_LIMIT)
        sig = jax.nn.sigmoid(SILU_ALPHA * gate_clip)
        act = gate_clip * sig
        hidden = ((up_clip + 1.0) * act).astype(BF16)
        d_up = jnp.where(jnp.abs(up_pre) < CLAMP_LIMIT, d_hidden * act, 0.0).astype(BF16)
        slope = sig + SILU_ALPHA * act * (1.0 - sig)
        d_gate = jnp.where(gate_pre < CLAMP_LIMIT, d_hidden * (up_clip + 1.0) * slope, 0.0).astype(BF16)
        for n, s in enumerate(blocks):
            hid_ref[s] = hidden[n * cap:(n + 1) * cap]
            dg_ref[s] = d_gate[n * cap:(n + 1) * cap]
            du_ref[s] = d_up[n * cap:(n + 1) * cap]

        def partial_of(q):
            at = pl.ds(pl.multiple_of(q * quarter, quarter), quarter)
            return cols_dot(d_gate, wg[at, :]) + cols_dot(d_up, wu[at, :])

        for yy in range(ny):
            psend[i, yy] = partial_of(yy * 2 + 1 - c).astype(BF16)
        remote(psend.at[i], precv.at[i], p_send.at[i], p_recv.at[i], partner).start()
        for yy in range(ny):
            pown[i % 2, yy] = partial_of(yy * 2 + c)

    def y_copy(i, n, yy, slot):
        return remote(
            ysend.at[i, n, yy], yrecv.at[i, n, slot], q_send.at[i, n, yy], q_recv.at[i, n, slot],
            (sp, tp_of(yy)),
        )

    def reduce_cores(i):
        remote(psend.at[i], precv.at[i], p_send.at[i], p_recv.at[i], partner).wait_recv()
        for n in (1, 0):
            at = slice(n * cap, (n + 1) * cap)
            for k in range(1, ny):
                yy = y_peer(k)
                ysend[i, n, yy] = (pown[i % 2, yy, at] + precv[i, yy, at].astype(F32)).astype(BF16)
                y_copy(i, n, yy, y).start()
        pown[i % 2, y] = pown[i % 2, y] + precv[i, y].astype(F32)

    def give_back(i):
        for n, s in ((1, far(-i)), (0, near(-i))):
            total = pown[i % 2, y, n * cap:(n + 1) * cap]
            for k in range(1, ny):
                yy = y_peer(k)
                y_copy(i, n, yy, yy).wait_recv()
                total = total + yrecv[i, n, yy].astype(F32)
            share[s] = total.astype(BF16)
            if n == 1:
                remote(share.at[s], comb.at[sp], r_send.at[s], r_recv.at[sp], (s, tp)).start()
            else:
                @pl.when(i > 0)
                def _():
                    remote(share.at[s], comb.at[sp], r_send.at[s], r_recv.at[sp], (s, tp)).start()

                @pl.when(i == 0)
                def _():
                    comb[sp] = share[sp]

    def flat(ref):
        return ref[...].reshape(slots, fh)

    def input_grads(q):
        left = x_ref[q, :, 0].reshape(slots, quarter).T
        at = slice(q * quarter, (q + 1) * quarter)
        gate_out[0, at, :] = rows_dot(left, flat(dg_ref))
        up_out[0, at, :] = rows_dot(left, flat(du_ref))

    def output_grads(q):
        at = slice(q * quarter, (q + 1) * quarter)
        down_out[0, :, at] = rows_dot(hid_t[...], x_ref[q, :, 1].reshape(slots, quarter))

    for load in late:
        load.wait()

    def step(i, carry):
        pl.when(i < half)(lambda: arrive(i))
        pl.when((i >= 2) & (i < half + 2))(lambda: compute(i - 2))
        pl.when((i >= 1) & (i < half + 1))(lambda: relay(i - 1))
        pl.when((i >= 2) & (i < half + 2))(lambda: reduce_cores(i - 2))
        pl.when(i == half)(spread_mirror)
        pl.when(i >= 3)(lambda: give_back(i - 3))
        return carry

    lax.fori_loop(0, half + 2, step, 0)
    hid_t[...] = flat(hid_ref).T
    output_grads(0)
    give_back(half - 1)
    for q in range(1, n_tp):
        output_grads(q)
    input_grads(0)

    def collect_from(d, acc):
        @pl.when(d != sp)
        def _():
            remote(share.at[d], comb.at[d], r_send.at[d], r_recv.at[d], (d, tp)).wait_recv()

        return acc + outer_dot(place[d], comb[d])

    def collect(r, acc):
        return collect_from(far(r), collect_from(near(r), acc))

    acc = lax.fori_loop(0, half, collect, cot_ref[:, own].astype(F32))
    token_grad = acc.astype(BF16)
    tg_ref[...] = token_grad
    tga[tp] = token_grad

    for k in range(1, ny):
        yy = y_peer(k)
        remote(tga.at[tp], tga.at[tp], ty_send.at[yy], ty_recv.at[y], (sp, tp_of(yy))).start()
    remote(tga.at[tp], tga.at[tp], tk_send.at[y], tk_recv.at[y], partner).start()
    input_grads(1)
    for k in range(1, ny):
        yy = y_peer(k)
        landed = tga.at[tp_of(yy)]
        remote(landed, landed, ty_send.at[yy], ty_recv.at[yy], (sp, tp_of(yy))).wait_recv()
        remote(landed, landed, tk_send.at[yy], tk_recv.at[yy], partner).start()
    for yy in range(ny):
        landed = tga.at[yy * 2 + 1 - c]
        remote(landed, landed, tk_send.at[yy], tk_recv.at[yy], partner).wait_recv()

    def feature_of(d):
        lane = (d * chunk) % quarter
        return tga.at[
            (d * chunk) // quarter,
            pl.ds(pl.multiple_of(c * part, part), part),
            pl.ds(pl.multiple_of(lane, chunk), chunk),
        ]

    d_conv = jnp.zeros((tok, chan), F32)
    for q in range(n_tp):
        d_conv += rows_dot(tga[q], outw[q * quarter:(q + 1) * quarter, :])
    back[...] = d_conv * gate_f
    halo_start(back, halo_b, 1)

    def send_features(r, carry):
        d = far(r)
        remote(feature_of(d), feat.at[c, sp], o_send.at[d], o_recv.at[sp], (d, tp)).start()

        @pl.when(r > 0)
        def _():
            e = near(r)
            remote(feature_of(e), feat.at[c, sp], o_send.at[e], o_recv.at[sp], (e, tp)).start()

        return carry

    lax.fori_loop(0, half, send_features, 0)
    feat[c, sp] = feature_of(sp)[...]

    gg_ref[...] = (d_conv * conv_s[...]).astype(BF16)
    for q in range(2, n_tp):
        input_grads(q)

    halo_finish(back, halo_b, 1)
    above, below = shifted(back[...], halo_b)
    d_prod = tap0 * below + tap1 * back[...] + tap2 * above
    cg_ref[...] = (d_prod * value_f).astype(BF16)
    vg_ref[...] = (d_prod * conv_f).astype(BF16)

    def land_features(r, carry):
        def wait_from(s):
            remote(feature_of(s), feat.at[c, s], o_send.at[s], o_recv.at[s], (s, tp)).wait_recv()

        wait_from(far(-r))
        pl.when(r > 0)(lambda: wait_from(near(-r)))
        return carry

    lax.fori_loop(0, half, land_features, 0)
    feat_copy = remote(feat.at[c], feat.at[c], ok_send.at[0], ok_recv.at[0], partner)
    feat_copy.start()

    def land_mixed(n, carry):
        s = (sp + n) % n_sp

        @pl.when(s != mirror)
        def _():
            mixed_copy(s, 0, s).wait_recv()

        return carry

    lax.fori_loop(1, n_sp, land_mixed, 0)

    def half_of(t):
        left = feat[t].reshape(n_sp * part, chunk)
        at = pl.ds(pl.multiple_of(t * part, part), part)
        right = mixed[:, at, :].reshape(n_sp * part, chan)
        return outer_dot(left, right)

    owg = half_of(c)
    feat_copy.wait_recv()
    owg_ref[...] = owg + half_of(1 - c)

    def drain(n, carry):
        d = (sp + n) % n_sp
        pl.when((d // half == side) & (d != sp))(
            lambda: remote(sendb.at[d], sendb.at[d], a_send.at[d], a_recv.at[d], (d, tp)).wait_send()
        )
        remote(share.at[d], share.at[d], r_send.at[d], r_recv.at[d], (d, tp)).wait_send()
        remote(feature_of(d), feat.at[c, sp], o_send.at[d], o_recv.at[d], (d, tp)).wait_send()
        for k in range(1, ny):
            yy = y_peer(k)
            mine = x_ref.at[tp, d]
            remote(mine, mine, y_send.at[yy, d], y_recv.at[yy, d], (sp, tp_of(yy))).wait_send()
        for yy in range(ny):
            mine = x_ref.at[tp_of(yy), d]
            remote(mine, mine, k_send.at[yy, d], k_recv.at[yy, d], partner).wait_send()
        return carry

    lax.fori_loop(1, n_sp, drain, 0)
    mixed_copy(sp, 0, mirror).wait_send()

    def drain_rounds(i, carry):
        remote(psend.at[i], precv.at[i], p_send.at[i], p_recv.at[i], partner).wait_send()
        for n in (1, 0):
            for k in range(1, ny):
                y_copy(i, n, y_peer(k), y).wait_send()

        @pl.when(i > 0)
        def _():
            mixed_copy(sp, 0, near(i)).wait_send()
            mixed_copy(mirror, 1, near(i)).wait_send()

        return carry

    lax.fori_loop(0, half, drain_rounds, 0)
    for k in range(1, ny):
        yy = y_peer(k)
        remote(tga.at[tp], tga.at[tp], ty_send.at[yy], ty_recv.at[y], (sp, tp_of(yy))).wait_send()
    for yy in range(ny):
        mine = tga.at[tp_of(yy)]
        remote(mine, mine, tk_send.at[yy], tk_recv.at[yy], partner).wait_send()
    feat_copy.wait_send()


def publish_kernel(*refs):
    count = len(refs) // 2
    copies = [
        pltpu.make_async_copy(refs[n], refs[count + n], refs[-1].at[n]) for n in range(count)
    ]
    for copy in copies:
        copy.start()
    for copy in copies:
        copy.wait()


def local_kernels(
    saved_tokens, cotangent, routes, route_weights, gate_in, conv_in, value_in, conv_taps,
    out_weight, gate_proj, up_proj, down_proj,
):
    tok, width = saved_tokens.shape
    n_sp, n_tp = lax.axis_size("sp"), lax.axis_size("tp")
    top = routes.shape[1]
    cap = 2 * tok * top // n_sp
    ny, half = n_tp // 2, n_sp // 2
    quarter = width // n_tp
    chan = gate_in.shape[1]
    fh = gate_proj.shape[2]
    chunk, part = width // n_sp, tok // 2
    rows = 2 * cap
    slots = n_sp * cap
    dims = (n_sp, n_tp, cap, quarter, tok, width, chan, fh)
    vmem = pl.BlockSpec(memory_space=pltpu.VMEM)
    hbm = pl.BlockSpec(memory_space=pltpu.HBM)
    dma = pltpu.SemaphoreType.DMA
    struct = jax.ShapeDtypeStruct
    def still(a):
        return pltpu.with_memory_space_constraint(a, pltpu.HBM)

    results = pl.pallas_call(
        functools.partial(exchange_kernel, dims),
        name="exchange",
        out_shape=(
            struct((1, width, fh), F32),
            struct((1, width, fh), F32),
            struct((1, fh, width), F32),
            struct((chunk, chan), F32),
            struct((tok, quarter), BF16),
            struct((tok, chan), BF16),
            struct((tok, chan), BF16),
            struct((tok, chan), BF16),
        ),
        in_specs=[hbm] * 12,
        out_specs=(vmem,) * 8,
        scratch_shapes=[
            pltpu.VMEM((n_tp, n_sp, 2, cap, quarter), BF16),
            pltpu.VMEM((n_sp, cap, fh), BF16),
            pltpu.VMEM((n_sp, cap, fh), BF16),
            pltpu.VMEM((n_sp, cap, fh), BF16),
            pltpu.VMEM((fh, slots), BF16),
            pltpu.VMEM((2, tok), jnp.int32),
            pltpu.VMEM((2, tok), F32),
            pltpu.VMEM((tok, width), BF16),
            pltpu.VMEM((tok, width), BF16),
            pltpu.VMEM((tok, chan), BF16),
            pltpu.VMEM((tok, chan), BF16),
            pltpu.VMEM((tok, chan), BF16),
            pltpu.VMEM(conv_taps.shape, F32),
            pltpu.VMEM((width, fh), BF16),
            pltpu.VMEM((width, fh), BF16),
            pltpu.VMEM((fh, width), BF16),
            pltpu.VMEM((width, chan), BF16),
            pltpu.VMEM((n_sp, cap, tok), BF16),
            pltpu.VMEM((n_sp, 2, cap, quarter), BF16),
            pltpu.VMEM((half, ny, rows, quarter), BF16),
            pltpu.VMEM((2, ny, rows, quarter), F32),
            pltpu.VMEM((half, ny, rows, quarter), BF16),
            pltpu.VMEM((half, 2, ny, cap, quarter), BF16),
            pltpu.VMEM((half, 2, ny, cap, quarter), BF16),
            pltpu.VMEM((n_sp, cap, quarter), BF16),
            pltpu.VMEM((n_sp, cap, quarter), BF16),
            pltpu.VMEM((n_tp, tok, quarter), BF16),
            pltpu.VMEM((tok, chan), F32),
            pltpu.VMEM((2, 8, chan), F32),
            pltpu.VMEM((tok, chan), F32),
            pltpu.VMEM((2, 8, chan), F32),
            pltpu.VMEM((tok, chan), F32),
            pltpu.VMEM((n_sp, tok, chan), BF16),
            pltpu.VMEM((2, n_sp, part, chunk), BF16),
            dma((n_sp,)), dma((n_sp,)),
            dma((ny, n_sp)), dma((ny, n_sp)),
            dma((ny, n_sp)), dma((ny, n_sp)),
            dma((half,)), dma((half,)),
            dma((half, 2, ny)), dma((half, 2, ny)),
            dma((n_sp,)), dma((n_sp,)),
            dma((ny,)), dma((ny,)),
            dma((ny,)), dma((ny,)),
            dma((2, 2)), dma((2, 2)),
            dma((2, n_sp)), dma((n_sp,)),
            dma((n_sp,)), dma((n_sp,)),
            dma((1,)), dma((1,)),
            dma((12,)),
        ],
        compiler_params=pltpu.CompilerParams(collective_id=0, has_side_effects=True, vmem_limit_bytes=39 << 20),
    )(
        *map(still, (
            routes.T, route_weights.T, saved_tokens, cotangent, gate_in, conv_in, value_in, conv_taps,
            out_weight, gate_proj, up_proj, down_proj,
        )),
    )
    return pl.pallas_call(
        publish_kernel,
        name="publish",
        out_shape=tuple(struct(a.shape, a.dtype) for a in results),
        in_specs=[vmem] * len(results),
        out_specs=(hbm,) * len(results),
        scratch_shapes=[dma((len(results),))],
        compiler_params=pltpu.CompilerParams(vmem_limit_bytes=16 << 20),
    )(*results)


def contract_rows(left, right):
    return lax.dot_general(
        left, right, (((0,), (0,)), ((), ())), preferred_element_type=jnp.float32
    )


def contract_cols(left, right):
    return lax.dot_general(
        left, right, (((1,), (1,)), ((), ())), preferred_element_type=jnp.float32
    )


def halo(cells, axis):
    count = lax.axis_size(axis)
    ends = count - 1
    above = lax.ppermute(cells[-1:], axis, [(i, (i + 1) % count) for i in range(ends)])
    below = lax.ppermute(cells[:1], axis, [((i + 1) % count, i) for i in range(ends)])
    return jnp.concatenate([above, cells, below], axis=0)


def exchange_groups(partial_value, part_width):
    tp_count = lax.axis_size("tp")
    pairs = tp_count // 2
    me = lax.axis_index("tp")
    side, pair = me % 2, me // 2

    def block(which_pair, which_side):
        return lax.dynamic_slice_in_dim(
            partial_value, (2 * which_pair + which_side) * part_width, part_width, 1
        )

    others = [(i, i ^ 1) for i in range(tp_count)]
    sums = []
    for step in range(1, pairs + 1):
        target = (pair + step) % pairs
        given = block(target, 1 - side).astype(jnp.bfloat16)
        got = lax.ppermute(given, "tp", others)
        sums.append(block(target, side) + got.astype(jnp.float32))
    total = sums[-1]
    for step in range(1, pairs):
        moves = [(i, (i + 2 * step) % tp_count) for i in range(tp_count)]
        got = lax.ppermute(sums[step - 1].astype(jnp.bfloat16), "tp", moves)
        total = total + got.astype(jnp.float32)
    return total


def gather_features(part):
    tp_count = lax.axis_size("tp")
    pairs = tp_count // 2
    me = lax.axis_index("tp")
    side, pair = me % 2, me // 2
    width = part.shape[1]
    others = [(i, i ^ 1) for i in range(tp_count)]
    held = [part]
    for step in range(1, pairs):
        moves = [(i, (i + 2 * step) % tp_count) for i in range(tp_count)]
        held.append(lax.ppermute(part, "tp", moves))
    twins = [lax.ppermute(block, "tp", others) for block in held]
    whole = jnp.zeros((part.shape[0], tp_count * width), part.dtype)
    for step in range(pairs):
        first = 2 * ((pair - step) % pairs)
        whole = lax.dynamic_update_slice_in_dim(whole, held[step], (first + side) * width, 1)
        whole = lax.dynamic_update_slice_in_dim(whole, twins[step], (first + 1 - side) * width, 1)
    return whole


def local_collectives(
    saved_tokens,
    cotangent,
    routes,
    route_weights,
    gate_in,
    conv_in,
    value_in,
    conv_taps,
    out_weight,
    gate_proj,
    up_proj,
    down_proj,
):
    tok_rows, model_width = saved_tokens.shape
    top_count = routes.shape[1]
    expert_count = lax.axis_size("sp")
    tp_count = lax.axis_size("tp")
    capacity = 2 * tok_rows * top_count // expert_count
    slots = expert_count * capacity
    part_width = model_width // tp_count
    channels = gate_in.shape[1]
    me_tp = lax.axis_index("tp")
    offset = me_tp * part_width

    routes_t = routes.T
    weights_t = route_weights.T
    experts = lax.broadcasted_iota(jnp.int32, (expert_count, tok_rows), 0)
    chosen = [experts == routes_t[k][None, :] for k in range(top_count)]
    hits = sum(c.astype(jnp.bfloat16) for c in chosen)
    earlier = (
        lax.broadcasted_iota(jnp.int32, (tok_rows, tok_rows), 0)
        < lax.broadcasted_iota(jnp.int32, (tok_rows, tok_rows), 1)
    ).astype(jnp.bfloat16)
    before = jnp.dot(hits, earlier, preferred_element_type=jnp.float32)
    slot_ids = lax.broadcasted_iota(jnp.int32, (slots, tok_rows), 0)
    place = jnp.zeros((slots, tok_rows), jnp.float32)
    weighted = jnp.zeros((slots, tok_rows), jnp.float32)
    for k in range(top_count):
        rank = jnp.sum(jnp.where(chosen[k], before, 0.0), axis=0).astype(jnp.int32)
        here = slot_ids == (routes_t[k] * capacity + rank)[None, :]
        place = jnp.where(here, 1.0, place)
        weighted = jnp.where(here, weights_t[k][None, :], weighted)
    place = place.astype(jnp.bfloat16)
    slot_weight = jnp.sum(weighted, axis=1, keepdims=True)

    own_tokens = lax.dynamic_slice_in_dim(saved_tokens, offset, part_width, 1)
    own_cot = lax.dynamic_slice_in_dim(cotangent, offset, part_width, 1)
    send_tokens = jnp.dot(place, own_tokens, preferred_element_type=jnp.float32).astype(jnp.bfloat16)
    cot_rows = jnp.dot(place, own_cot, preferred_element_type=jnp.float32)
    send_grads = (cot_rows * slot_weight).astype(jnp.bfloat16)

    def dispatched(rows):
        rows = rows.reshape(expert_count, capacity, part_width)
        return lax.all_to_all(rows, "sp", split_axis=0, concat_axis=0, tiled=True)

    arrived_tokens = dispatched(send_tokens)
    arrived_tokens, send_grads = lax.optimization_barrier((arrived_tokens, send_grads))
    arrived_grads = dispatched(send_grads)
    rows_in = gather_features(arrived_tokens.reshape(slots, part_width))
    grads_in = gather_features(arrived_grads.reshape(slots, part_width))

    gate_f32 = gate_in.astype(jnp.float32)
    conv_f32 = conv_in.astype(jnp.float32)
    value_f32 = value_in.astype(jnp.float32)
    my_taps = lax.dynamic_slice_in_dim(conv_taps, me_tp * channels, channels, 1)
    prod_rim = halo(conv_f32 * value_f32, "sp")
    conv_out = my_taps[0] * prod_rim[:-2] + my_taps[1] * prod_rim[1:-1] + my_taps[2] * prod_rim[2:]
    mixed = (gate_f32 * conv_out).astype(jnp.bfloat16)
    mixed = jnp.concatenate([mixed, mixed], axis=1)

    w_gate, w_up, w_down = gate_proj[0], up_proj[0], down_proj[0]
    gate_pre = jnp.dot(rows_in, w_gate, preferred_element_type=jnp.float32)
    up_pre = jnp.dot(rows_in, w_up, preferred_element_type=jnp.float32)
    gate_clip = jnp.minimum(gate_pre, CLAMP_LIMIT)
    up_clip = jnp.clip(up_pre, -CLAMP_LIMIT, CLAMP_LIMIT)
    sigmoid_gate = jax.nn.sigmoid(SILU_ALPHA * gate_clip)
    gated_act = gate_clip * sigmoid_gate
    hidden = ((up_clip + 1.0) * gated_act).astype(jnp.bfloat16)
    grads_in, mixed = lax.optimization_barrier((grads_in, mixed))
    mixed_all = lax.all_gather(mixed, "sp", axis=0, tiled=True)
    d_hidden = contract_cols(grads_in, w_down)
    d_up = jnp.where(jnp.abs(up_pre) < CLAMP_LIMIT, d_hidden * gated_act, 0.0).astype(jnp.bfloat16)
    gate_slope = sigmoid_gate + SILU_ALPHA * gate_clip * sigmoid_gate * (1.0 - sigmoid_gate)
    d_gate = jnp.where(gate_pre < CLAMP_LIMIT, d_hidden * (up_clip + 1.0) * gate_slope, 0.0).astype(
        jnp.bfloat16
    )
    partial_value = contract_cols(d_gate, w_gate) + contract_cols(d_up, w_up)
    shares = exchange_groups(partial_value, part_width).astype(jnp.bfloat16)
    down_grad = contract_rows(hidden, grads_in)
    gate_grad = contract_rows(rows_in, d_gate)
    up_grad = contract_rows(rows_in, d_up)

    returned = dispatched(shares).reshape(slots, part_width)
    combined = contract_rows(place, returned)
    token_grad = (own_cot.astype(jnp.float32) + combined).astype(jnp.bfloat16)
    residual = lax.all_gather(token_grad, "tp", axis=1, tiled=True)

    d_conv_out = jnp.dot(residual, out_weight, preferred_element_type=jnp.float32)
    grad_rim = halo(d_conv_out * gate_f32, "sp")
    d_product = my_taps[0] * grad_rim[2:] + my_taps[1] * grad_rim[1:-1] + my_taps[2] * grad_rim[:-2]
    gate_in_grad = (d_conv_out * conv_out).astype(jnp.bfloat16)
    conv_in_grad = (d_product * value_f32).astype(jnp.bfloat16)
    value_in_grad = (d_product * conv_f32).astype(jnp.bfloat16)

    share = tok_rows // tp_count
    quarter = lax.dynamic_slice_in_dim(residual, me_tp * share, share, 0)
    quarter = quarter.reshape(share, expert_count, model_width // expert_count)
    quarter = lax.all_to_all(
        quarter.transpose(1, 0, 2), "sp", split_axis=0, concat_axis=0, tiled=True
    )
    features = lax.all_gather(quarter, "tp", axis=1, tiled=True)
    features = features.reshape(expert_count * tok_rows, -1)
    out_weight_grad = contract_rows(features, mixed_all[:, :channels])
    return (
        gate_grad[None],
        up_grad[None],
        down_grad[None],
        out_weight_grad,
        token_grad,
        gate_in_grad,
        conv_in_grad,
        value_in_grad,
    )


def local(*arrays):
    tok, width = arrays[0].shape
    n_sp, n_tp = lax.axis_size("sp"), lax.axis_size("tp")
    cap = 2 * tok * arrays[2].shape[1] // n_sp
    aligned = (
        arrays[2].shape[1] == 2
        and n_tp % 2 == 0
        and cap % 16 == 0
        and n_sp % 2 == 0
        and tok % 32 == 0
        and width % (128 * n_sp) == 0
        and n_sp % n_tp == 0
    )
    return (local_kernels if aligned else local_collectives)(*arrays)


def solution(mesh):
    in_specs = (
        P("sp", None),
        P("sp", None),
        P("sp", None),
        P("sp", None),
        P("sp", "tp"),
        P("sp", "tp"),
        P("sp", "tp"),
        P(),
        P(None, "tp"),
        P("sp", None, "tp"),
        P("sp", None, "tp"),
        P("sp", "tp", None),
    )
    out_specs = (
        P("sp", None, "tp"),
        P("sp", None, "tp"),
        P("sp", "tp", None),
        P("sp", "tp"),
        P("sp", "tp"),
        P("sp", "tp"),
        P("sp", "tp"),
        P("sp", "tp"),
    )
    return jax.shard_map(local, mesh=mesh, in_specs=in_specs, out_specs=out_specs, check_vma=False)
```

```python
import functools

import jax
import jax.numpy as jnp
from jax import lax
from jax.experimental import pallas as pl
from jax.experimental.pallas import tpu as pltpu
from jax.sharding import PartitionSpec as P

CLAMP_LIMIT = 7.0
SILU_ALPHA = 1.702
AHEAD = 2
MESH = pl.DeviceIdType.MESH
BF16 = jnp.bfloat16
F32 = jnp.float32


def dot(left, right, dims):
    return lax.dot_general(left, right, (dims, ((), ())), preferred_element_type=F32)


def rows_dot(left, right):
    return dot(left, right, ((1,), (0,)))


def cols_dot(left, right):
    return dot(left, right, ((1,), (1,)))


def outer_dot(left, right):
    return dot(left, right, ((0,), (0,)))


def exchange_kernel(
    dims,
    routes_hbm, weights_hbm, tokens_hbm, cot_hbm, gate_hbm, conv_hbm, value_hbm, taps_hbm,
    outw_hbm, wg_hbm, wu_hbm, wd_hbm,
    gate_out, up_out, down_out, owg_ref, tg_ref, gg_ref, cg_ref, vg_ref,
    x_ref, hid_ref, dg_ref, du_ref, hid_t,
    routes_ref, weights_ref, tokens_ref, cot_ref, gate_ref, conv_ref, value_ref, taps_ref,
    wg, wu, wd, outw, place, sendb, psend, pown, precv, ysend, yrecv, share, comb,
    tga, prod, halo_p, back, halo_b, conv_s, mixed, feat,
    a_send, a_recv, y_send, y_recv, k_send, k_recv, p_send, p_recv, q_send, q_recv,
    r_send, r_recv, ty_send, ty_recv, tk_send, tk_recv, h_send, h_recv, m_send, m_recv,
    o_send, o_recv, ok_send, ok_recv, l_sem,
):
    n_sp, n_tp, cap, quarter, tok, width, chan, fh = dims
    ny = n_tp // 2
    half = n_sp // 2
    slots = n_sp * cap
    chunk = width // n_sp
    part = tok // 2
    sp, tp = lax.axis_index("sp"), lax.axis_index("tp")
    side, pos = sp // half, sp % half
    mirror = (1 - side) * half + pos
    y, c = tp // 2, tp % 2
    partner = (sp, y * 2 + 1 - c)

    def near(r):
        return side * half + (pos + half + r) % half

    def far(r):
        return (1 - side) * half + (pos + half + r) % half

    def tp_of(yy):
        return yy * 2 + c

    def y_peer(k):
        return (y + k) % ny

    def remote(src, dst, ssem, rsem, dev):
        return pltpu.make_async_remote_copy(
            src_ref=src, dst_ref=dst, send_sem=ssem, recv_sem=rsem,
            device_id=dev, device_id_type=MESH,
        )

    barrier = pltpu.get_barrier_semaphore()

    def greet(n, carry):
        pl.semaphore_signal(barrier, inc=1, device_id=((sp + n) % n_sp, tp), device_id_type=MESH)
        return carry

    lax.fori_loop(1, n_sp, greet, 0)
    for k in range(1, ny):
        pl.semaphore_signal(barrier, inc=1, device_id=(sp, tp_of(y_peer(k))), device_id_type=MESH)
    pl.semaphore_signal(barrier, inc=1, device_id=partner, device_id_type=MESH)

    sources = (
        routes_hbm, weights_hbm, tokens_hbm, cot_hbm, gate_hbm, conv_hbm, value_hbm, taps_hbm,
        wg_hbm.at[0], wu_hbm.at[0], wd_hbm.at[0], outw_hbm,
    )
    targets = (
        routes_ref, weights_ref, tokens_ref, cot_ref, gate_ref, conv_ref, value_ref, taps_ref,
        wg, wu, wd, outw,
    )
    loads = [
        pltpu.make_async_copy(source, target, l_sem.at[n])
        for n, (source, target) in enumerate(zip(sources, targets))
    ]
    early, late = loads[2:8], loads[8:]
    for load in loads:
        load.start()

    loads[0].wait()
    loads[1].wait()
    experts = lax.broadcasted_iota(jnp.int32, (n_sp, tok), 0)
    first, second = routes_ref[0:1, :], routes_ref[1:2, :]
    hit_a, hit_b = experts == first, experts == second
    hits = jnp.where(hit_a, 1.0, 0.0) + jnp.where(hit_b, 1.0, 0.0)
    earlier = (
        lax.broadcasted_iota(jnp.int32, (tok, tok), 0) < lax.broadcasted_iota(jnp.int32, (tok, tok), 1)
    )
    before = rows_dot(hits.astype(BF16), jnp.where(earlier, 1.0, 0.0).astype(BF16))

    def slot_of(hit, named):
        rank = jnp.sum(jnp.where(hit, before, 0.0), axis=0, keepdims=True).astype(jnp.int32)
        return named * cap + rank

    slot_a, slot_b = slot_of(hit_a, first), slot_of(hit_b, second)
    weight_a, weight_b = weights_ref[0:1, :], weights_ref[1:2, :]
    slot_iota = lax.broadcasted_iota(jnp.int32, (cap, tok), 0)
    own = pl.ds(pl.multiple_of(tp * quarter, quarter), quarter)

    def placed(d):
        here_a = slot_iota + d * cap == slot_a
        here_b = slot_iota + d * cap == slot_b
        picked = jnp.where(here_a, 1.0, jnp.where(here_b, 1.0, 0.0)).astype(BF16)
        scale = jnp.sum(
            jnp.where(here_a, weight_a, jnp.where(here_b, weight_b, 0.0)), axis=1, keepdims=True
        )
        place[d] = picked
        return picked, scale

    def block_copy(d, yy):
        return remote(
            sendb.at[d, yy], x_ref.at[tp_of(yy), sp], a_send.at[d, yy], a_recv.at[sp, yy], (d, tp)
        )

    def block_landing(s, yy):
        landed = x_ref.at[tp_of(yy), s]
        return remote(landed, landed, a_send.at[s, yy], a_recv.at[s, yy], (s, tp))

    def send_block(d, features):
        picked, scale = placed(d)
        for k in features:
            yy = y_peer(k)
            at = pl.ds(pl.multiple_of(tp_of(yy) * quarter, quarter), quarter)
            sendb[d, yy, 0] = rows_dot(picked, tokens_ref[:, at]).astype(BF16)
            sendb[d, yy, 1] = (rows_dot(picked, cot_ref[:, at]) * scale).astype(BF16)
            block_copy(d, yy).start()

    for load in early:
        load.wait()
    gate_f = gate_ref[...].astype(F32)
    conv_f = conv_ref[...].astype(F32)
    value_f = value_ref[...].astype(F32)
    prod[...] = conv_f * value_f
    up_dev, down_dev = ((sp + 1) % n_sp, tp), ((sp + n_sp - 1) % n_sp, tp)

    def halo_copies(source, landing, which):
        to_next = remote(
            source.at[pl.ds(tok - 8, 8)], landing.at[0], h_send.at[which, 0], h_recv.at[which, 0], up_dev
        )
        to_prev = remote(
            source.at[pl.ds(0, 8)], landing.at[1], h_send.at[which, 1], h_recv.at[which, 1], down_dev
        )
        return to_next, to_prev

    def halo_start(source, landing, which):
        to_next, to_prev = halo_copies(source, landing, which)

        @pl.when(sp < n_sp - 1)
        def _():
            to_next.start()

        @pl.when(sp == n_sp - 1)
        def _():
            landing[1] = jnp.zeros(landing.shape[1:], F32)

        @pl.when(sp > 0)
        def _():
            to_prev.start()

        @pl.when(sp == 0)
        def _():
            landing[0] = jnp.zeros(landing.shape[1:], F32)

    def halo_finish(source, landing, which):
        to_next, to_prev = halo_copies(source, landing, which)

        @pl.when(sp < n_sp - 1)
        def _():
            to_next.wait_send()
            to_prev.wait_recv()

        @pl.when(sp > 0)
        def _():
            to_prev.wait_send()
            to_next.wait_recv()

    def shifted(cells, landing):
        at_row = lax.broadcasted_iota(jnp.int32, cells.shape, 0)
        above = jnp.where(at_row == 0, landing[0, 7:8, :], pltpu.roll(cells, 1, 0))
        below = jnp.where(at_row == tok - 1, landing[1, 0:1, :], pltpu.roll(cells, tok - 1, 0))
        return above, below

    pl.semaphore_wait(barrier, (n_sp - 1) + (ny - 1) + 1)
    halo_start(prod, halo_p, 0)
    tap_at = pl.ds(pl.multiple_of(tp * chan, chan), chan)
    tap0, tap1, tap2 = taps_ref[0:1, tap_at], taps_ref[1:2, tap_at], taps_ref[2:3, tap_at]


    def dispatch(r):
        send_block(far(r), range(1))
        pl.when(r + 1 < half)(lambda: send_block(near(r + 1), range(ny)))

    def dispatched(r):
        block_copy(far(r), y).wait_send()

    for r in range(min(AHEAD, half)):
        dispatch(r)

    picked, scale = placed(sp)
    for q in range(n_tp):
        at = slice(q * quarter, (q + 1) * quarter)
        x_ref[q, sp, 0] = rows_dot(picked, tokens_ref[:, at]).astype(BF16)
        x_ref[q, sp, 1] = (rows_dot(picked, cot_ref[:, at]) * scale).astype(BF16)

    def mixed_copy(b, which, d):
        return remote(mixed.at[b], mixed.at[b], m_send.at[which, d], m_recv.at[b], (d, tp))

    def spread_own():
        halo_finish(prod, halo_p, 0)
        above, below = shifted(prod[...], halo_p)
        conv_out = tap0 * above + tap1 * prod[...] + tap2 * below
        conv_s[...] = conv_out
        mixed[sp] = (gate_f * conv_out).astype(BF16)
        mixed_copy(sp, 0, mirror).start()

        def one(r, carry):
            mixed_copy(sp, 0, near(r)).start()
            return carry

        lax.fori_loop(1, half, one, 0)

    def spread_mirror():
        mixed_copy(mirror, 0, mirror).wait_recv()

        def one(r, carry):
            mixed_copy(mirror, 1, near(r)).start()
            return carry

        lax.fori_loop(1, half, one, 0)

    def to_partner(yy, s):
        landed = x_ref.at[tp_of(yy), s]
        return remote(landed, landed, k_send.at[yy, s], k_recv.at[yy, s], partner)

    def to_y_peer(yy, s):
        landed = x_ref.at[tp, s]
        return remote(landed, landed, y_send.at[yy, s], y_recv.at[y, s], (sp, tp_of(yy)))

    def land_near(s):
        for k in range(ny):
            block_landing(s, y_peer(k)).wait_recv()
            to_partner(y_peer(k), s).start()

    def land_far(s):
        block_landing(s, y).wait_recv()
        for k in range(1, ny):
            to_y_peer(y_peer(k), s).start()
        to_partner(y, s).start()

    def arrive(i):
        dispatched(i)
        pl.when(i + AHEAD < half)(lambda: dispatch(i + AHEAD))
        pl.when(i == half - 1)(spread_own)
        pl.when(i + 1 < half)(lambda: land_near(near(-i - 1)))
        land_far(far(-i))

    def relay(i):
        s = far(-i)
        for k in range(1, ny):
            yy = y_peer(k)
            landed = x_ref.at[tp_of(yy), s]
            remote(landed, landed, y_send.at[yy, s], y_recv.at[yy, s], (sp, tp_of(yy))).wait_recv()
            to_partner(yy, s).start()

    def complete(s):
        for yy in range(ny):
            landed = x_ref.at[yy * 2 + 1 - c, s]
            remote(landed, landed, k_send.at[yy, s], k_recv.at[yy, s], partner).wait_recv()

    def compute(i):
        blocks = (near(-i), far(-i))
        pl.when(i > 0)(lambda: complete(blocks[0]))
        complete(blocks[1])

        def cells(q, which):
            return jnp.concatenate([x_ref[q, s, which] for s in blocks], axis=0)

        rows = 2 * cap
        gate_pre = jnp.zeros((rows, fh), F32)
        up_pre = jnp.zeros((rows, fh), F32)
        d_hidden = jnp.zeros((rows, fh), F32)
        for q in range(n_tp):
            gate_pre += rows_dot(cells(q, 0), wg[q * quarter:(q + 1) * quarter, :])
            up_pre += rows_dot(cells(q, 0), wu[q * quarter:(q + 1) * quarter, :])
        for q in range(n_tp):
            d_hidden += cols_dot(cells(q, 1), wd[:, q * quarter:(q + 1) * quarter])
        gate_clip = jnp.minimum(gate_pre, CLAMP_LIMIT)
        up_clip = jnp.clip(up_pre, -CLAMP_LIMIT, CLAMP_LIMIT)
        sig = jax.nn.sigmoid(SILU_ALPHA * gate_clip)
        act = gate_clip * sig
        hidden = ((up_clip + 1.0) * act).astype(BF16)
        d_up = jnp.where(jnp.abs(up_pre) < CLAMP_LIMIT, d_hidden * act, 0.0).astype(BF16)
        slope = sig + SILU_ALPHA * act * (1.0 - sig)
        d_gate = jnp.where(gate_pre < CLAMP_LIMIT, d_hidden * (up_clip + 1.0) * slope, 0.0).astype(BF16)
        for n, s in enumerate(blocks):
            hid_ref[s] = hidden[n * cap:(n + 1) * cap]
            dg_ref[s] = d_gate[n * cap:(n + 1) * cap]
            du_ref[s] = d_up[n * cap:(n + 1) * cap]

        def partial_of(q):
            at = pl.ds(pl.multiple_of(q * quarter, quarter), quarter)
            return cols_dot(d_gate, wg[at, :]) + cols_dot(d_up, wu[at, :])

        for yy in range(ny):
            psend[i, yy] = partial_of(yy * 2 + 1 - c).astype(BF16)
        remote(psend.at[i], precv.at[i], p_send.at[i], p_recv.at[i], partner).start()
        for yy in range(ny):
            pown[i % 2, yy] = partial_of(yy * 2 + c)

    def y_copy(i, n, yy, slot):
        return remote(
            ysend.at[i, n, yy], yrecv.at[i, n, slot], q_send.at[i, n, yy], q_recv.at[i, n, slot],
            (sp, tp_of(yy)),
        )

    def reduce_cores(i):
        remote(psend.at[i], precv.at[i], p_send.at[i], p_recv.at[i], partner).wait_recv()
        for n in (1, 0):
            at = slice(n * cap, (n + 1) * cap)
            for k in range(1, ny):
                yy = y_peer(k)
                ysend[i, n, yy] = (pown[i % 2, yy, at] + precv[i, yy, at].astype(F32)).astype(BF16)
                y_copy(i, n, yy, y).start()
        pown[i % 2, y] = pown[i % 2, y] + precv[i, y].astype(F32)

    def give_back(i):
        for n, s in ((1, far(-i)), (0, near(-i))):
            total = pown[i % 2, y, n * cap:(n + 1) * cap]
            for k in range(1, ny):
                yy = y_peer(k)
                y_copy(i, n, yy, yy).wait_recv()
                total = total + yrecv[i, n, yy].astype(F32)
            share[s] = total.astype(BF16)
            if n == 1:
                remote(share.at[s], comb.at[sp], r_send.at[s], r_recv.at[sp], (s, tp)).start()
            else:
                @pl.when(i > 0)
                def _():
                    remote(share.at[s], comb.at[sp], r_send.at[s], r_recv.at[sp], (s, tp)).start()

                @pl.when(i == 0)
                def _():
                    comb[sp] = share[sp]

    def flat(ref):
        return ref[...].reshape(slots, fh)

    def input_grads(q):
        left = x_ref[q, :, 0].reshape(slots, quarter).T
        at = slice(q * quarter, (q + 1) * quarter)
        gate_out[0, at, :] = rows_dot(left, flat(dg_ref))
        up_out[0, at, :] = rows_dot(left, flat(du_ref))

    def output_grads(q):
        at = slice(q * quarter, (q + 1) * quarter)
        down_out[0, :, at] = rows_dot(hid_t[...], x_ref[q, :, 1].reshape(slots, quarter))

    for load in late:
        load.wait()

    def step(i, carry):
        pl.when(i < half)(lambda: arrive(i))
        pl.when((i >= 2) & (i < half + 2))(lambda: compute(i - 2))
        pl.when((i >= 1) & (i < half + 1))(lambda: relay(i - 1))
        pl.when((i >= 2) & (i < half + 2))(lambda: reduce_cores(i - 2))
        pl.when(i >= 3)(lambda: give_back(i - 3))
        return carry

    lax.fori_loop(0, half + 2, step, 0)
    hid_t[...] = flat(hid_ref).T
    output_grads(0)
    give_back(half - 1)
    for q in range(1, n_tp):
        output_grads(q)
    input_grads(0)

    def collect_from(d, acc):
        @pl.when(d != sp)
        def _():
            remote(share.at[d], comb.at[d], r_send.at[d], r_recv.at[d], (d, tp)).wait_recv()

        return acc + outer_dot(place[d], comb[d])

    def collect(r, acc):
        return collect_from(far(r), collect_from(near(r), acc))

    acc = lax.fori_loop(0, half, collect, cot_ref[:, own].astype(F32))
    token_grad = acc.astype(BF16)
    tg_ref[...] = token_grad
    tga[tp] = token_grad

    for k in range(1, ny):
        yy = y_peer(k)
        remote(tga.at[tp], tga.at[tp], ty_send.at[yy], ty_recv.at[y], (sp, tp_of(yy))).start()
    remote(tga.at[tp], tga.at[tp], tk_send.at[y], tk_recv.at[y], partner).start()
    spread_mirror()
    input_grads(1)
    for k in range(1, ny):
        yy = y_peer(k)
        landed = tga.at[tp_of(yy)]
        remote(landed, landed, ty_send.at[yy], ty_recv.at[yy], (sp, tp_of(yy))).wait_recv()
        remote(landed, landed, tk_send.at[yy], tk_recv.at[yy], partner).start()
    for yy in range(ny):
        landed = tga.at[yy * 2 + 1 - c]
        remote(landed, landed, tk_send.at[yy], tk_recv.at[yy], partner).wait_recv()

    def feature_of(d):
        lane = (d * chunk) % quarter
        return tga.at[
            (d * chunk) // quarter,
            pl.ds(pl.multiple_of(c * part, part), part),
            pl.ds(pl.multiple_of(lane, chunk), chunk),
        ]

    d_conv = jnp.zeros((tok, chan), F32)
    for q in range(n_tp):
        d_conv += rows_dot(tga[q], outw[q * quarter:(q + 1) * quarter, :])
    back[...] = d_conv * gate_f
    halo_start(back, halo_b, 1)

    def send_features(r, carry):
        d = far(r)
        remote(feature_of(d), feat.at[c, sp], o_send.at[d], o_recv.at[sp], (d, tp)).start()

        @pl.when(r > 0)
        def _():
            e = near(r)
            remote(feature_of(e), feat.at[c, sp], o_send.at[e], o_recv.at[sp], (e, tp)).start()

        return carry

    lax.fori_loop(0, half, send_features, 0)
    feat[c, sp] = feature_of(sp)[...]

    gg_ref[...] = (d_conv * conv_s[...]).astype(BF16)
    for q in range(2, n_tp):
        input_grads(q)

    halo_finish(back, halo_b, 1)
    above, below = shifted(back[...], halo_b)
    d_prod = tap0 * below + tap1 * back[...] + tap2 * above
    cg_ref[...] = (d_prod * value_f).astype(BF16)
    vg_ref[...] = (d_prod * conv_f).astype(BF16)

    def land_features(r, carry):
        def wait_from(s):
            remote(feature_of(s), feat.at[c, s], o_send.at[s], o_recv.at[s], (s, tp)).wait_recv()

        wait_from(far(-r))
        pl.when(r > 0)(lambda: wait_from(near(-r)))
        return carry

    lax.fori_loop(0, half, land_features, 0)
    feat_copy = remote(feat.at[c], feat.at[c], ok_send.at[0], ok_recv.at[0], partner)
    feat_copy.start()

    def land_mixed(n, carry):
        s = (sp + n) % n_sp

        @pl.when(s != mirror)
        def _():
            mixed_copy(s, 0, s).wait_recv()

        return carry

    lax.fori_loop(1, n_sp, land_mixed, 0)

    def half_of(t):
        left = feat[t].reshape(n_sp * part, chunk)
        at = pl.ds(pl.multiple_of(t * part, part), part)
        right = mixed[:, at, :].reshape(n_sp * part, chan)
        return outer_dot(left, right)

    owg = half_of(c)
    feat_copy.wait_recv()
    owg_ref[...] = owg + half_of(1 - c)

    def drain(n, carry):
        d = (sp + n) % n_sp
        beside = d // half == side

        @pl.when(beside)
        def _():
            for yy in range(ny):
                block_copy(d, yy).wait_send()

        @pl.when(jnp.logical_not(beside))
        def _():
            for k in range(1, ny):
                to_y_peer(y_peer(k), d).wait_send()

        for yy in range(ny):
            to_partner(yy, d).wait_send()
        remote(share.at[d], share.at[d], r_send.at[d], r_recv.at[d], (d, tp)).wait_send()
        remote(feature_of(d), feat.at[c, sp], o_send.at[d], o_recv.at[d], (d, tp)).wait_send()
        return carry

    lax.fori_loop(1, n_sp, drain, 0)
    mixed_copy(sp, 0, mirror).wait_send()

    def drain_rounds(i, carry):
        remote(psend.at[i], precv.at[i], p_send.at[i], p_recv.at[i], partner).wait_send()
        for n in (1, 0):
            for k in range(1, ny):
                y_copy(i, n, y_peer(k), y).wait_send()

        @pl.when(i > 0)
        def _():
            mixed_copy(sp, 0, near(i)).wait_send()
            mixed_copy(mirror, 1, near(i)).wait_send()

        return carry

    lax.fori_loop(0, half, drain_rounds, 0)
    for k in range(1, ny):
        yy = y_peer(k)
        remote(tga.at[tp], tga.at[tp], ty_send.at[yy], ty_recv.at[y], (sp, tp_of(yy))).wait_send()
    for yy in range(ny):
        mine = tga.at[tp_of(yy)]
        remote(mine, mine, tk_send.at[yy], tk_recv.at[yy], partner).wait_send()
    feat_copy.wait_send()


def publish_kernel(*refs):
    count = len(refs) // 2
    copies = [
        pltpu.make_async_copy(refs[n], refs[count + n], refs[-1].at[n]) for n in range(count)
    ]
    for copy in copies:
        copy.start()
    for copy in copies:
        copy.wait()


def local_kernels(
    saved_tokens, cotangent, routes, route_weights, gate_in, conv_in, value_in, conv_taps,
    out_weight, gate_proj, up_proj, down_proj,
):
    tok, width = saved_tokens.shape
    n_sp, n_tp = lax.axis_size("sp"), lax.axis_size("tp")
    top = routes.shape[1]
    cap = 2 * tok * top // n_sp
    ny, half = n_tp // 2, n_sp // 2
    quarter = width // n_tp
    chan = gate_in.shape[1]
    fh = gate_proj.shape[2]
    chunk, part = width // n_sp, tok // 2
    rows = 2 * cap
    slots = n_sp * cap
    dims = (n_sp, n_tp, cap, quarter, tok, width, chan, fh)
    vmem = pl.BlockSpec(memory_space=pltpu.VMEM)
    hbm = pl.BlockSpec(memory_space=pltpu.HBM)
    dma = pltpu.SemaphoreType.DMA
    struct = jax.ShapeDtypeStruct
    def still(a):
        return pltpu.with_memory_space_constraint(a, pltpu.HBM)

    results = pl.pallas_call(
        functools.partial(exchange_kernel, dims),
        name="exchange",
        out_shape=(
            struct((1, width, fh), F32),
            struct((1, width, fh), F32),
            struct((1, fh, width), F32),
            struct((chunk, chan), F32),
            struct((tok, quarter), BF16),
            struct((tok, chan), BF16),
            struct((tok, chan), BF16),
            struct((tok, chan), BF16),
        ),
        in_specs=[hbm] * 12,
        out_specs=(vmem,) * 8,
        scratch_shapes=[
            pltpu.VMEM((n_tp, n_sp, 2, cap, quarter), BF16),
            pltpu.VMEM((n_sp, cap, fh), BF16),
            pltpu.VMEM((n_sp, cap, fh), BF16),
            pltpu.VMEM((n_sp, cap, fh), BF16),
            pltpu.VMEM((fh, slots), BF16),
            pltpu.VMEM((2, tok), jnp.int32),
            pltpu.VMEM((2, tok), F32),
            pltpu.VMEM((tok, width), BF16),
            pltpu.VMEM((tok, width), BF16),
            pltpu.VMEM((tok, chan), BF16),
            pltpu.VMEM((tok, chan), BF16),
            pltpu.VMEM((tok, chan), BF16),
            pltpu.VMEM(conv_taps.shape, F32),
            pltpu.VMEM((width, fh), BF16),
            pltpu.VMEM((width, fh), BF16),
            pltpu.VMEM((fh, width), BF16),
            pltpu.VMEM((width, chan), BF16),
            pltpu.VMEM((n_sp, cap, tok), BF16),
            pltpu.VMEM((n_sp, ny, 2, cap, quarter), BF16),
            pltpu.VMEM((half, ny, rows, quarter), BF16),
            pltpu.VMEM((2, ny, rows, quarter), F32),
            pltpu.VMEM((half, ny, rows, quarter), BF16),
            pltpu.VMEM((half, 2, ny, cap, quarter), BF16),
            pltpu.VMEM((half, 2, ny, cap, quarter), BF16),
            pltpu.VMEM((n_sp, cap, quarter), BF16),
            pltpu.VMEM((n_sp, cap, quarter), BF16),
            pltpu.VMEM((n_tp, tok, quarter), BF16),
            pltpu.VMEM((tok, chan), F32),
            pltpu.VMEM((2, 8, chan), F32),
            pltpu.VMEM((tok, chan), F32),
            pltpu.VMEM((2, 8, chan), F32),
            pltpu.VMEM((tok, chan), F32),
            pltpu.VMEM((n_sp, tok, chan), BF16),
            pltpu.VMEM((2, n_sp, part, chunk), BF16),
            dma((n_sp, ny)), dma((n_sp, ny)),
            dma((ny, n_sp)), dma((ny, n_sp)),
            dma((ny, n_sp)), dma((ny, n_sp)),
            dma((half,)), dma((half,)),
            dma((half, 2, ny)), dma((half, 2, ny)),
            dma((n_sp,)), dma((n_sp,)),
            dma((ny,)), dma((ny,)),
            dma((ny,)), dma((ny,)),
            dma((2, 2)), dma((2, 2)),
            dma((2, n_sp)), dma((n_sp,)),
            dma((n_sp,)), dma((n_sp,)),
            dma((1,)), dma((1,)),
            dma((12,)),
        ],
        compiler_params=pltpu.CompilerParams(collective_id=0, has_side_effects=True, vmem_limit_bytes=41 << 20),
    )(
        *map(still, (
            routes.T, route_weights.T, saved_tokens, cotangent, gate_in, conv_in, value_in, conv_taps,
            out_weight, gate_proj, up_proj, down_proj,
        )),
    )
    return pl.pallas_call(
        publish_kernel,
        name="publish",
        out_shape=tuple(struct(a.shape, a.dtype) for a in results),
        in_specs=[vmem] * len(results),
        out_specs=(hbm,) * len(results),
        scratch_shapes=[dma((len(results),))],
        compiler_params=pltpu.CompilerParams(vmem_limit_bytes=16 << 20),
    )(*results)


def contract_rows(left, right):
    return lax.dot_general(
        left, right, (((0,), (0,)), ((), ())), preferred_element_type=jnp.float32
    )


def contract_cols(left, right):
    return lax.dot_general(
        left, right, (((1,), (1,)), ((), ())), preferred_element_type=jnp.float32
    )


def halo(cells, axis):
    count = lax.axis_size(axis)
    ends = count - 1
    above = lax.ppermute(cells[-1:], axis, [(i, (i + 1) % count) for i in range(ends)])
    below = lax.ppermute(cells[:1], axis, [((i + 1) % count, i) for i in range(ends)])
    return jnp.concatenate([above, cells, below], axis=0)


def exchange_groups(partial_value, part_width):
    tp_count = lax.axis_size("tp")
    pairs = tp_count // 2
    me = lax.axis_index("tp")
    side, pair = me % 2, me // 2

    def block(which_pair, which_side):
        return lax.dynamic_slice_in_dim(
            partial_value, (2 * which_pair + which_side) * part_width, part_width, 1
        )

    others = [(i, i ^ 1) for i in range(tp_count)]
    sums = []
    for step in range(1, pairs + 1):
        target = (pair + step) % pairs
        given = block(target, 1 - side).astype(jnp.bfloat16)
        got = lax.ppermute(given, "tp", others)
        sums.append(block(target, side) + got.astype(jnp.float32))
    total = sums[-1]
    for step in range(1, pairs):
        moves = [(i, (i + 2 * step) % tp_count) for i in range(tp_count)]
        got = lax.ppermute(sums[step - 1].astype(jnp.bfloat16), "tp", moves)
        total = total + got.astype(jnp.float32)
    return total


def gather_features(part):
    tp_count = lax.axis_size("tp")
    pairs = tp_count // 2
    me = lax.axis_index("tp")
    side, pair = me % 2, me // 2
    width = part.shape[1]
    others = [(i, i ^ 1) for i in range(tp_count)]
    held = [part]
    for step in range(1, pairs):
        moves = [(i, (i + 2 * step) % tp_count) for i in range(tp_count)]
        held.append(lax.ppermute(part, "tp", moves))
    twins = [lax.ppermute(block, "tp", others) for block in held]
    whole = jnp.zeros((part.shape[0], tp_count * width), part.dtype)
    for step in range(pairs):
        first = 2 * ((pair - step) % pairs)
        whole = lax.dynamic_update_slice_in_dim(whole, held[step], (first + side) * width, 1)
        whole = lax.dynamic_update_slice_in_dim(whole, twins[step], (first + 1 - side) * width, 1)
    return whole


def local_collectives(
    saved_tokens,
    cotangent,
    routes,
    route_weights,
    gate_in,
    conv_in,
    value_in,
    conv_taps,
    out_weight,
    gate_proj,
    up_proj,
    down_proj,
):
    tok_rows, model_width = saved_tokens.shape
    top_count = routes.shape[1]
    expert_count = lax.axis_size("sp")
    tp_count = lax.axis_size("tp")
    capacity = 2 * tok_rows * top_count // expert_count
    slots = expert_count * capacity
    part_width = model_width // tp_count
    channels = gate_in.shape[1]
    me_tp = lax.axis_index("tp")
    offset = me_tp * part_width

    routes_t = routes.T
    weights_t = route_weights.T
    experts = lax.broadcasted_iota(jnp.int32, (expert_count, tok_rows), 0)
    chosen = [experts == routes_t[k][None, :] for k in range(top_count)]
    hits = sum(c.astype(jnp.bfloat16) for c in chosen)
    earlier = (
        lax.broadcasted_iota(jnp.int32, (tok_rows, tok_rows), 0)
        < lax.broadcasted_iota(jnp.int32, (tok_rows, tok_rows), 1)
    ).astype(jnp.bfloat16)
    before = jnp.dot(hits, earlier, preferred_element_type=jnp.float32)
    slot_ids = lax.broadcasted_iota(jnp.int32, (slots, tok_rows), 0)
    place = jnp.zeros((slots, tok_rows), jnp.float32)
    weighted = jnp.zeros((slots, tok_rows), jnp.float32)
    for k in range(top_count):
        rank = jnp.sum(jnp.where(chosen[k], before, 0.0), axis=0).astype(jnp.int32)
        here = slot_ids == (routes_t[k] * capacity + rank)[None, :]
        place = jnp.where(here, 1.0, place)
        weighted = jnp.where(here, weights_t[k][None, :], weighted)
    place = place.astype(jnp.bfloat16)
    slot_weight = jnp.sum(weighted, axis=1, keepdims=True)

    own_tokens = lax.dynamic_slice_in_dim(saved_tokens, offset, part_width, 1)
    own_cot = lax.dynamic_slice_in_dim(cotangent, offset, part_width, 1)
    send_tokens = jnp.dot(place, own_tokens, preferred_element_type=jnp.float32).astype(jnp.bfloat16)
    cot_rows = jnp.dot(place, own_cot, preferred_element_type=jnp.float32)
    send_grads = (cot_rows * slot_weight).astype(jnp.bfloat16)

    def dispatched(rows):
        rows = rows.reshape(expert_count, capacity, part_width)
        return lax.all_to_all(rows, "sp", split_axis=0, concat_axis=0, tiled=True)

    arrived_tokens = dispatched(send_tokens)
    arrived_tokens, send_grads = lax.optimization_barrier((arrived_tokens, send_grads))
    arrived_grads = dispatched(send_grads)
    rows_in = gather_features(arrived_tokens.reshape(slots, part_width))
    grads_in = gather_features(arrived_grads.reshape(slots, part_width))

    gate_f32 = gate_in.astype(jnp.float32)
    conv_f32 = conv_in.astype(jnp.float32)
    value_f32 = value_in.astype(jnp.float32)
    my_taps = lax.dynamic_slice_in_dim(conv_taps, me_tp * channels, channels, 1)
    prod_rim = halo(conv_f32 * value_f32, "sp")
    conv_out = my_taps[0] * prod_rim[:-2] + my_taps[1] * prod_rim[1:-1] + my_taps[2] * prod_rim[2:]
    mixed = (gate_f32 * conv_out).astype(jnp.bfloat16)
    mixed = jnp.concatenate([mixed, mixed], axis=1)

    w_gate, w_up, w_down = gate_proj[0], up_proj[0], down_proj[0]
    gate_pre = jnp.dot(rows_in, w_gate, preferred_element_type=jnp.float32)
    up_pre = jnp.dot(rows_in, w_up, preferred_element_type=jnp.float32)
    gate_clip = jnp.minimum(gate_pre, CLAMP_LIMIT)
    up_clip = jnp.clip(up_pre, -CLAMP_LIMIT, CLAMP_LIMIT)
    sigmoid_gate = jax.nn.sigmoid(SILU_ALPHA * gate_clip)
    gated_act = gate_clip * sigmoid_gate
    hidden = ((up_clip + 1.0) * gated_act).astype(jnp.bfloat16)
    grads_in, mixed = lax.optimization_barrier((grads_in, mixed))
    mixed_all = lax.all_gather(mixed, "sp", axis=0, tiled=True)
    d_hidden = contract_cols(grads_in, w_down)
    d_up = jnp.where(jnp.abs(up_pre) < CLAMP_LIMIT, d_hidden * gated_act, 0.0).astype(jnp.bfloat16)
    gate_slope = sigmoid_gate + SILU_ALPHA * gate_clip * sigmoid_gate * (1.0 - sigmoid_gate)
    d_gate = jnp.where(gate_pre < CLAMP_LIMIT, d_hidden * (up_clip + 1.0) * gate_slope, 0.0).astype(
        jnp.bfloat16
    )
    partial_value = contract_cols(d_gate, w_gate) + contract_cols(d_up, w_up)
    shares = exchange_groups(partial_value, part_width).astype(jnp.bfloat16)
    down_grad = contract_rows(hidden, grads_in)
    gate_grad = contract_rows(rows_in, d_gate)
    up_grad = contract_rows(rows_in, d_up)

    returned = dispatched(shares).reshape(slots, part_width)
    combined = contract_rows(place, returned)
    token_grad = (own_cot.astype(jnp.float32) + combined).astype(jnp.bfloat16)
    residual = lax.all_gather(token_grad, "tp", axis=1, tiled=True)

    d_conv_out = jnp.dot(residual, out_weight, preferred_element_type=jnp.float32)
    grad_rim = halo(d_conv_out * gate_f32, "sp")
    d_product = my_taps[0] * grad_rim[2:] + my_taps[1] * grad_rim[1:-1] + my_taps[2] * grad_rim[:-2]
    gate_in_grad = (d_conv_out * conv_out).astype(jnp.bfloat16)
    conv_in_grad = (d_product * value_f32).astype(jnp.bfloat16)
    value_in_grad = (d_product * conv_f32).astype(jnp.bfloat16)

    share = tok_rows // tp_count
    quarter = lax.dynamic_slice_in_dim(residual, me_tp * share, share, 0)
    quarter = quarter.reshape(share, expert_count, model_width // expert_count)
    quarter = lax.all_to_all(
        quarter.transpose(1, 0, 2), "sp", split_axis=0, concat_axis=0, tiled=True
    )
    features = lax.all_gather(quarter, "tp", axis=1, tiled=True)
    features = features.reshape(expert_count * tok_rows, -1)
    out_weight_grad = contract_rows(features, mixed_all[:, :channels])
    return (
        gate_grad[None],
        up_grad[None],
        down_grad[None],
        out_weight_grad,
        token_grad,
        gate_in_grad,
        conv_in_grad,
        value_in_grad,
    )


def local(*arrays):
    tok, width = arrays[0].shape
    n_sp, n_tp = lax.axis_size("sp"), lax.axis_size("tp")
    cap = 2 * tok * arrays[2].shape[1] // n_sp
    aligned = (
        arrays[2].shape[1] == 2
        and n_tp % 2 == 0
        and cap % 16 == 0
        and n_sp % 2 == 0
        and tok % 32 == 0
        and width % (128 * n_sp) == 0
        and n_sp % n_tp == 0
    )
    return (local_kernels if aligned else local_collectives)(*arrays)


def solution(mesh):
    in_specs = (
        P("sp", None),
        P("sp", None),
        P("sp", None),
        P("sp", None),
        P("sp", "tp"),
        P("sp", "tp"),
        P("sp", "tp"),
        P(),
        P(None, "tp"),
        P("sp", None, "tp"),
        P("sp", None, "tp"),
        P("sp", "tp", None),
    )
    out_specs = (
        P("sp", None, "tp"),
        P("sp", None, "tp"),
        P("sp", "tp", None),
        P("sp", "tp"),
        P("sp", "tp"),
        P("sp", "tp"),
        P("sp", "tp"),
        P("sp", "tp"),
    )
    return jax.shard_map(local, mesh=mesh, in_specs=in_specs, out_specs=out_specs, check_vma=False)
```
